32 devices in a mesh: sp: 8 (over z, y), dp: 4 (over x, core).
Axes of the slice: x: 2, y: 2, z: 4, core: 2. Of those that a mesh axis runs over, the one named last changes fastest.
Arguments:
- gated: bfloat16 [4, 1024, 3072], P('dp', 'sp'), may hold values from -6 to 6
- values_in: bfloat16 [4, 1024, 3072], P('dp', 'sp'), may hold values from -6 to 6
- upstream: bfloat16 [4, 1024, 3072], P('dp', 'sp'), may hold values from -6 to 6
- gain: float32 [3072], replicated, may hold values from 0.1 to 1.9
- shift: float32 [3072], replicated, may hold values from -3 to 3
- mix_w: bfloat16 [512, 4, 512], P('dp'), may hold values from -0.375 to 0.375
- mix_bias: float32 [4, 512], replicated, may hold values from 0.1 to 1.9
Outputs:
- grad_u: bfloat16 [4, 1024, 3072], P('dp', 'sp')
- grad_v: bfloat16 [4, 1024, 3072], P('dp', 'sp')
- grad_mix: float32 [512, 4, 512], P('dp')
- grad_bias: float32 [4, 512], replicated
- grad_gain: float32 [3072], replicated
- grad_shift: float32 [3072], replicated
The draws below stay inside these ranges and needn't reach their ends.
All inputs are finite; a program needn't handle non-finite values.
Results may differ from the reference program's by a relative error of at most 0.014.
Values may be sent and summed in bfloat16 or wider, within the bound.
A program may use at most 64 MiB of HBM per device.

```python
import jax
import jax.numpy as jnp
from jax import lax

GROUPS = 4
GROUP_DIM = 768
SPAN = 512
SEG = 64
HALF = 3072
LENGTH = 1024
BATCH = 4


def level_of(own_key, extent, shards, smallest, top_value):
    def one(dim, parts):
        steps = jax.random.uniform(jax.random.fold_in(jax.random.fold_in(own_key, 6), dim), (parts,), jnp.float32, smallest / len(shards), top_value / len(shards))
        return jnp.repeat(jnp.exp(steps), extent[dim] // parts).reshape((-1,) + (1,) * (len(extent) - dim - 1))

    loudness = one(*shards[0])
    for cut in shards[1:]:
        loudness = loudness * one(*cut)
    return loudness


def noise(rng, dims, deviation, most, split=(), kind=jnp.bfloat16):
    loudness = level_of(rng, dims, split, -0.22, 0.18) if split else 1.0
    drawn = jax.random.normal(rng, dims, jnp.float32) * deviation * loudness
    return jnp.minimum(jnp.maximum(drawn, -most), most).astype(kind)


def setup_inputs(seed: int = 0) -> dict:
    streams_of = jax.random.split(jax.random.key(seed), 8)
    gated = noise(streams_of[0], (BATCH, LENGTH, HALF), 1.0, 6.0, ((0, 4), (1, 8)))
    values_in = noise(streams_of[1], (BATCH, LENGTH, HALF), 1.0, 6.0, ((0, 4), (1, 8)))
    upstream = noise(streams_of[2], (BATCH, LENGTH, HALF), 1.0, 6.0, ((0, 4), (1, 8)))
    gain = jnp.clip(1.0 + 0.18 * jax.random.normal(streams_of[3], (HALF,), jnp.float32), 0.1, 1.9)
    shift = noise(streams_of[4], (HALF,), 0.5, 3.0, (), jnp.float32)
    mix_w = noise(streams_of[5], (SPAN, GROUPS, SPAN), (SPAN // 2) ** -0.5, 0.375, ((0, 4),))
    mix_bias = jnp.clip(1.0 + 0.18 * jax.random.normal(streams_of[6], (GROUPS, SPAN), jnp.float32), 0.1, 1.9)
    return {"gated": gated, "values_in": values_in, "upstream": upstream, "gain": gain, "shift": shift, "mix_w": mix_w, "mix_bias": mix_bias}


EPS = 1e-05

def span_mask():
    places = jnp.arange(SPAN)
    return (places[:, None] // SEG >= places[None, :] // SEG).astype(jnp.float32)

def reference(gated, values_in, upstream, gain, shift, mix_w, mix_bias):
    allowed = span_mask()
    masked_w = mix_w.astype(jnp.float32) * allowed[:, None, :]
    blocks = LENGTH // SPAN

    def one_sequence(carry, inputs):
        gated_row, values_row, upstream_row = inputs
        raw_values = values_row.astype(jnp.float32)
        centred = raw_values - lax.optimization_barrier(jnp.mean(raw_values, axis=-1, keepdims=True))
        inv_std = lax.rsqrt(lax.optimization_barrier(jnp.mean(centred * centred, axis=-1, keepdims=True)) + EPS)
        unit_v = centred * inv_std
        normed = (unit_v * gain + shift).astype(jnp.bfloat16)
        mix_grad = (upstream_row.astype(jnp.float32) * gated_row.astype(jnp.float32)).astype(jnp.bfloat16)
        norm_blocks = normed.reshape(blocks, SPAN, GROUPS, GROUP_DIM).astype(jnp.float32)
        grad_blocks = mix_grad.reshape(blocks, SPAN, GROUPS, GROUP_DIM).astype(jnp.float32)
        mixed_f = jnp.einsum('tgs,nsgc->ntgc', masked_w, norm_blocks) + mix_bias.T[None, :, :, None]
        mixed = lax.optimization_barrier(mixed_f.astype(jnp.bfloat16)).reshape(LENGTH, HALF)
        grad_u = (upstream_row.astype(jnp.float32) * mixed.astype(jnp.float32)).astype(jnp.bfloat16)
        back_f = jnp.einsum('tgs,ntgc->nsgc', masked_w, grad_blocks)
        grad_normed = lax.optimization_barrier(back_f.astype(jnp.bfloat16)).reshape(LENGTH, HALF).astype(jnp.float32)
        scaled = grad_normed * gain
        grad_v = inv_std * (scaled - lax.optimization_barrier(jnp.mean(scaled, axis=-1, keepdims=True)) - unit_v * lax.optimization_barrier(jnp.mean(scaled * unit_v, axis=-1, keepdims=True)))
        mix_term = jnp.einsum('ntgc,nsgc->tgs', grad_blocks, norm_blocks) * allowed[:, None, :]
        bias_term = lax.optimization_barrier(jnp.sum(grad_blocks, axis=(0, 3))).T
        carry = (carry[0] + mix_term, carry[1] + bias_term, carry[2] + lax.optimization_barrier(jnp.sum(grad_normed * unit_v, axis=0)), carry[3] + lax.optimization_barrier(jnp.sum(grad_normed, axis=0)))
        return (carry, (grad_u, grad_v.astype(jnp.bfloat16)))
    initial = (jnp.zeros((SPAN, GROUPS, SPAN), jnp.float32), jnp.zeros((GROUPS, SPAN), jnp.float32), jnp.zeros((HALF,), jnp.float32), jnp.zeros((HALF,), jnp.float32))
    totals, outputs = lax.scan(one_sequence, initial, (gated, values_in, upstream))
    return (outputs[0], outputs[1], totals[0], totals[1], totals[2], totals[3])
```

```python
import functools

import jax
import jax.numpy as jnp
from jax import lax
from jax.experimental import pallas as pl
from jax.experimental.pallas import tpu as pltpu
from jax.sharding import PartitionSpec as P

SEG = 64

EPS = 1e-05

CHUNK = 16

QUAD = 4


def nt(a, b):
    return lax.dot_general(a, b, (((1,), (1,)), ((), ())), preferred_element_type=jnp.float32)


def tn(a, b):
    return lax.dot_general(a, b, (((0,), (0,)), ((), ())), preferred_element_type=jnp.float32)


def nn(a, b):
    return jnp.dot(a, b, preferred_element_type=jnp.float32)


def kernel(
    dims,
    gated_in,
    values_in,
    upstream_in,
    gain,
    shift,
    mix_in,
    mix_bias,
    grad_u,
    grad_v,
    grad_mix,
    summed,
    gated,
    values,
    upstream,
    mix_w,
    unit,
    inv,
    nbuf,
    gbuf,
    w_send,
    w_block,
    stage_y,
    stage_z,
    recv_y,
    recv_z,
    own_part,
    back,
    sum_a,
    sum_b,
    acc_gain,
    acc_shift,
    term_w,
    term_n,
    red_w,
    red_n,
    dp_w,
    dp_n,
    span_w,
    span_n,
    all_w,
    all_n,
    vec_a,
    vec_b,
    vec_c,
    vec_s,
    bias_t,
    raw_sems,
    part_sems,
    dp_send,
    dp_recv,
    sn_send,
    sn_recv,
    sq_send,
    sq_recv,
    in_sem,
):
    tok, width, groups, span, dp_count, spans = dims
    half = groups * width
    rows = span // dp_count
    per_block = tok // rows
    hg = groups // 2
    me = lax.axis_index("sp")
    my_span, k = me // QUAD, lax.rem(me, QUAD)
    zb, yb = k // 2, lax.rem(k, 2)
    d = lax.axis_index("dp")
    t_own = d // per_block
    f32, bf16 = jnp.float32, jnp.bfloat16

    def sq_id(j):
        return {"sp": my_span * QUAD + j}

    def dp_id(j):
        return {"dp": j}

    def sn_id(j):
        return {"sp": j * QUAD + k}

    y_id = sq_id(k + 1 - 2 * yb)
    z_id = sq_id(k + 2 - 4 * zb)

    def remote(src, dst, send, recv, where):
        return pltpu.make_async_remote_copy(
            src_ref=src,
            dst_ref=dst,
            send_sem=send,
            recv_sem=recv,
            device_id=where,
            device_id_type=pl.DeviceIdType.MESH,
        )

    class Exchange:
        def __init__(self, src, dst, own, count, where, send, recv, slot, gives=None, takes=None):
            self.src, self.dst, self.own, self.count = src, dst, own, count
            self.where, self.send, self.recv, self.slot = where, send, recv, slot
            self.gives, self.takes = gives, takes

        def copy(self, step, to):
            peer = lax.rem(self.own + step, self.count)
            landing = self.own if to else peer
            return remote(
                self.src(peer) if to else self.dst(landing),
                self.dst(landing),
                self.send.at[self.slot, step],
                self.recv.at[self.slot, landing],
                self.where(peer),
            )

        def each(self, cond, act):
            for step in range(1, self.count):
                if cond is None:
                    act(step)
                else:
                    pl.when(cond(lax.rem(self.own + step, self.count)))(lambda: act(step))

        def start(self):
            self.each(self.gives, lambda step: self.copy(step, True).start())

        def arrive(self):
            self.each(self.takes, lambda step: self.copy(step, False).wait_recv())

        def leave(self):
            self.each(self.gives, lambda step: self.copy(step, True).wait_send())

    def square(src, dst, slot, gives=None, takes=None):
        return Exchange(src, dst, k, QUAD, sq_id, sq_send, sq_recv, slot, gives, takes)

    def across(src, dst, slot, gives=None, takes=None):
        return Exchange(src, dst, d, dp_count, dp_id, dp_send, dp_recv, slot, gives, takes)

    def spanning(src, dst, slot, gives=None, takes=None):
        return Exchange(src, dst, my_span, spans, sn_id, sn_send, sn_recv, slot, gives, takes)

    fetches = [
        pltpu.make_async_copy(src, dst, in_sem.at[i])
        for i, (src, dst) in enumerate(
            (
                (gated_in, gated),
                (upstream_in, upstream),
                (values_in, values),
                (mix_in, mix_w),
            )
        )
    ]
    for fetch in (fetches[2], fetches[0], fetches[1], fetches[3]):
        fetch.start()

    barrier = pltpu.get_barrier_semaphore()
    for own, count, where in (
        (k, QUAD, sq_id),
        (d, dp_count, dp_id),
        (my_span, spans, sn_id),
    ):
        for step in range(1, count):
            pl.semaphore_signal(
                barrier,
                inc=1,
                device_id=where(lax.rem(own + step, count)),
                device_id_type=pl.DeviceIdType.MESH,
            )

    def piece(r):
        return pl.ds(pl.multiple_of(r * CHUNK, CHUNK), CHUNK)

    def lanes_of(g):
        return slice(g * width, (g + 1) * width)

    def allowed(first_t, first_s, n_t, n_s):
        t = first_t + lax.broadcasted_iota(jnp.int32, (n_t, n_s), 0)
        s = first_s + lax.broadcasted_iota(jnp.int32, (n_t, n_s), 1)
        return lax.div(t, SEG) >= lax.div(s, SEG)

    def run(z):
        first = range(hg)
        second = range(hg, groups)
        wide = first if z == 0 else second
        narrow = second if z == 0 else first
        n_own = {g: yb if (z == 0 or g in first) else 1 for g in range(groups)}
        g_own = {g: yb if (z == 1 or g in second) else 0 for g in range(groups)}

        def makes_w(t):
            return (lax.rem(t, 2) == yb) if z == 0 else (t >= 2)

        def slot_w(t):
            return lax.div(t, 2) if z == 0 else t - 2

        def makes_n(t):
            return t == k

        def of(j):
            return j // per_block

        def part(j):
            return lax.rem(j, per_block)

        x_buf = nbuf if z == 0 else gbuf
        o_buf = gbuf if z == 0 else nbuf
        raw_y = {}
        for g in wide:
            raw_y[g] = x_buf
        y_send = {
            g: remote(
                x_buf.at[g, yb], x_buf.at[g, yb], raw_sems.at[0, g], raw_sems.at[1, g], y_id
            )
            for g in wide
        }
        y_take = {
            g: remote(
                x_buf.at[g, 1 - yb],
                x_buf.at[g, 1 - yb],
                raw_sems.at[0, g],
                raw_sems.at[1, g],
                y_id,
            )
            for g in wide
        }

        def narrow_y(buf, slot, g):
            return remote(
                buf.at[g, slot], buf.at[g, slot], raw_sems.at[0, g], raw_sems.at[1, g], y_id
            )

        z_buf = nbuf if z == 0 else gbuf
        z_own = n_own if z == 0 else g_own
        z_slot = 0 if z == 0 else 1
        z_send = {
            g: remote(
                z_buf.at[g, z_own[g]],
                z_buf.at[g, z_slot],
                raw_sems.at[2, g],
                raw_sems.at[3, g],
                z_id,
            )
            for g in narrow
        }
        z_take = {
            g: remote(
                o_buf.at[g, 1 - z_slot],
                o_buf.at[g, 1 - z_slot],
                raw_sems.at[2, g],
                raw_sems.at[3, g],
                z_id,
            )
            for g in wide
        }
        py = [
            remote(stage_y.at[i], recv_y.at[i], part_sems.at[0, i], part_sems.at[1, i], y_id)
            for i in range(hg)
        ]
        pz = [
            remote(stage_z.at[i], recv_z.at[i], part_sems.at[2, i], part_sems.at[3, i], z_id)
            for i in range(hg)
        ]

        def needs(h):
            return makes_w if h == z else ((lambda t: t < 2) if z == 0 else (lambda t: t >= 2))

        def slot_of(h, t):
            return slot_w(t) if h == z else (t if z == 0 else t - 2)

        def w_at(h, j):
            return w_block.at[slot_of(h, of(j)) * per_block + part(j), h * hg : (h + 1) * hg]

        go_mix = [
            across(
                lambda j, h=h: w_send.at[h * hg : (h + 1) * hg],
                lambda j, h=h: w_at(h, j),
                h,
                lambda j, h=h: needs(h)(t_own),
                lambda j, h=h: needs(h)(of(j)),
            )
            for h in range(2)
        ]
        go_tw = across(
            lambda j: term_w.at[slot_w(of(j)) * per_block + part(j)],
            lambda j: red_w.at[j],
            2,
            lambda j: makes_w(of(j)),
            lambda j: makes_w(t_own),
        )
        go_tn = across(
            lambda j: term_n.at[part(j)],
            lambda j: red_n.at[j],
            3,
            lambda j: makes_n(of(j)),
            lambda j: makes_n(t_own),
        )
        go_sw = spanning(
            lambda j: dp_w,
            lambda j: span_w.at[j],
            0,
            lambda j: makes_w(t_own),
            lambda j: makes_w(t_own),
        )
        go_sn = spanning(
            lambda j: dp_n,
            lambda j: span_n.at[j],
            1,
            lambda j: makes_n(t_own),
            lambda j: makes_n(t_own),
        )

        def peer_w(j):
            return ((j < 2) & (lax.rem(t_own, 2) == j)) | ((j >= 2) & (t_own >= 2))

        go_aw = square(
            lambda j: all_w.at[k],
            lambda j: all_w.at[j],
            0,
            lambda j: makes_w(t_own),
            peer_w,
        )
        go_an = square(
            lambda j: all_n.at[k],
            lambda j: all_n.at[j],
            1,
            lambda j: makes_n(t_own),
            lambda j: t_own == j,
        )
        go_va = across(lambda j: vec_s.at[0], lambda j: vec_a.at[j], 4)
        go_vb = square(lambda j: vec_s.at[1], lambda j: vec_b.at[j], 2)
        go_vc = spanning(lambda j: vec_s.at[2], lambda j: vec_c.at[j], 2)

        def make_normed():
            fetches[2].wait()

            @pl.loop(0, tok // CHUNK)
            def _(r):
                at = piece(r)
                raw = values[at, :].astype(f32)
                centred = raw - jnp.mean(raw, axis=-1, keepdims=True)
                inv_std = lax.rsqrt(jnp.mean(centred * centred, axis=-1, keepdims=True) + EPS)
                one = centred * inv_std
                unit[at, :] = one
                inv[at, :] = jnp.broadcast_to(inv_std, (CHUNK, 128))
                normed = (one * gain[...] + shift[...]).astype(bf16)
                for g in range(groups):
                    nbuf[g, n_own[g], at, :] = normed[:, lanes_of(g)]

        def make_cotangent():
            fetches[0].wait()
            fetches[1].wait()

            @pl.loop(0, tok // CHUNK)
            def _(r):
                at = piece(r)
                prod = (upstream[at, :].astype(f32) * gated[at, :].astype(f32)).astype(bf16)
                for g in range(groups):
                    gbuf[g, g_own[g], at, :] = prod[:, lanes_of(g)]

        def meet():
            pl.semaphore_wait(barrier, QUAD + dp_count + spans - 3)

        def narrow_n():
            @pl.when(yb == 0)
            def _():
                for g in narrow:
                    narrow_y(nbuf, 0, g).start()

        def narrow_g():
            @pl.when(yb == 1)
            def _():
                for g in narrow:
                    narrow_y(gbuf, 1, g).start()

        (make_normed if z == 0 else make_cotangent)()
        meet()
        for g, h in zip(wide, narrow):
            y_send[g].start()
            z_send[h].start()
        (narrow_n if z == 0 else narrow_g)()
        (make_cotangent if z == 0 else make_normed)()
        (narrow_g if z == 0 else narrow_n)()

        @pl.when(yb == 0)
        def _():
            for g in narrow:
                nbuf[g, 1] = jnp.zeros((tok, width), bf16)

        @pl.when(yb == 1)
        def _():
            for g in narrow:
                gbuf[g, 0] = jnp.zeros((tok, width), bf16)

        fetches[3].wait()

        @pl.loop(0, rows // CHUNK)
        def _(r):
            at = piece(r)
            for c in range(2):
                for h in range(2):
                    if z == 0:
                        col = c
                    elif h == 0:
                        col = 2 + c
                    else:
                        col = yb + 2 * c
                    start = col * tok
                    if not isinstance(start, int):
                        start = pl.multiple_of(start, tok)
                    block = mix_w[at, :, pl.ds(start, tok)].astype(f32)
                    keep = allowed(d * rows + r * CHUNK, col * tok, CHUNK, tok)
                    for g in range(h * hg, (h + 1) * hg):
                        w_send[g, at, c * tok : (c + 1) * tok] = jnp.where(
                            keep, block[:, g, :], 0.0
                        ).astype(bf16)

        for h in (z, 1 - z):
            go_mix[h].start()

            @pl.when(needs(h)(t_own))
            def _():
                w_at(h, d)[...] = w_send[h * hg : (h + 1) * hg]

        own_bias = mix_bias[:, 0:tok]
        for b in range(1, QUAD):
            own_bias = jnp.where(k == b, mix_bias[:, b * tok : (b + 1) * tok], own_bias)
        for g in range(groups):
            bias_t[g] = jnp.transpose(jnp.broadcast_to(own_bias[g : g + 1], (128, tok)))
        acc_gain[...] = jnp.zeros_like(acc_gain)
        acc_shift[...] = jnp.zeros_like(acc_shift)
        sum_a[...] = jnp.zeros_like(sum_a)
        sum_b[...] = jnp.zeros_like(sum_b)
        grad_mix[...] = jnp.zeros_like(grad_mix)
        parts = half // span
        for g in range(groups):
            bias_sum = nt(jnp.ones((8, width), bf16), gbuf[g, g_own[g]])[0:1]
            at = 2 * parts + g
            for b in range(QUAD):
                vec_s[0, at : at + 1, b * tok : (b + 1) * tok] = jnp.where(k == b, bias_sum, 0.0)

        def give_u(g, mixed):
            for c in range(width // 128):
                lanes = slice(c * 128, (c + 1) * 128)
                at = slice(g * width + c * 128, g * width + (c + 1) * 128)
                whole = (mixed[:, lanes] + bias_t[g]).astype(bf16).astype(f32)
                grad_u[:, at] = (upstream[:, at].astype(f32) * whole).astype(bf16)

        def give_back(g, total):
            back[g] = total.astype(bf16)

            @pl.loop(0, tok // CHUNK)
            def _(r):
                at = piece(r)
                grad_normed = back[g, at, :].astype(f32)
                one = unit[at, lanes_of(g)]
                prod = grad_normed * one
                acc_gain[:, lanes_of(g)] += prod[0:8] + prod[8:16]
                acc_shift[:, lanes_of(g)] += grad_normed[0:8] + grad_normed[8:16]
                scaled = grad_normed * gain[:, lanes_of(g)]
                prod = scaled * one
                a, b = scaled[:, 0:128], prod[:, 0:128]
                for c in range(1, width // 128):
                    a = a + scaled[:, c * 128 : (c + 1) * 128]
                    b = b + prod[:, c * 128 : (c + 1) * 128]
                sum_a[at, :] += a
                sum_b[at, :] += b

        def give_v():
            @pl.loop(0, tok // CHUNK)
            def _(r):
                at = piece(r)
                mean_a = jnp.sum(sum_a[at, :], axis=-1, keepdims=True) / half
                mean_b = jnp.sum(sum_b[at, :], axis=-1, keepdims=True) / half
                inv_std = inv[at, :][:, 0:1]
                for g in range(groups):
                    scaled = back[g, at, :].astype(f32) * gain[:, lanes_of(g)]
                    grad_v[at, lanes_of(g)] = (
                        inv_std * (scaled - mean_a - unit[at, lanes_of(g)] * mean_b)
                    ).astype(bf16)

        def own_cols(g, block):
            at = pl.ds(pl.multiple_of(block * tok, tok), tok)
            return w_block[:, g, :, at].reshape(2 * tok, tok)

        def own_rows(g, block):
            return w_block[pl.ds(block * per_block, per_block), g].reshape(tok, 2 * tok)

        def pair(buf, g):
            return buf[g].reshape(2 * tok, width)

        go_mix[z].arrive()
        for i, g in enumerate(wide):
            y_take[g].wait_recv()
            if z == 0:
                both = nn(w_block[:, g].reshape(2 * tok, 2 * tok), pair(nbuf, g))
                stage_z[i] = both[tok:].astype(bf16)
                pz[i].start()
                give_u(g, both[:tok])
            else:
                both = tn(w_block[:, g].reshape(2 * tok, 2 * tok), pair(gbuf, g))
                stage_z[i] = both[:tok].astype(bf16)
                pz[i].start()
                give_back(g, both[tok:])
        for i, g in enumerate(wide):
            z_take[g].wait_recv()
            if z == 0:
                stage_y[i] = tn(own_cols(g, 1 - yb), pair(gbuf, g)).astype(bf16)
                py[i].start()
                own_part[i] = tn(own_cols(g, yb), pair(gbuf, g))
            else:
                stage_y[i] = nn(own_rows(g, 1 - yb), pair(nbuf, g)).astype(bf16)
                py[i].start()
                own_part[i] = nn(own_rows(g, yb), pair(nbuf, g))

        def keep_of(row, col):
            return allowed(row * tok, col * tok, tok, tok)

        for i, g in enumerate(wide):
            block = nt(pair(gbuf, g), pair(nbuf, g))
            for a in range(2):
                for b in range(2):
                    if z == 0:
                        keep = keep_of(yb + 2 * a, b)
                    else:
                        keep = keep_of(2 + a, yb + 2 * b)
                    at, of_s = slice(a * tok, (a + 1) * tok), slice(b * tok, (b + 1) * tok)
                    kept = jnp.where(keep, block[at, of_s], 0.0).astype(bf16)
                    for p in range(per_block):
                        term_w[a * per_block + p, i, :, of_s] = kept[p * rows : (p + 1) * rows]
        go_tw.start()

        go_mix[1 - z].arrive()
        for i, g in enumerate(narrow):

            @pl.when(yb == 1)
            def _():
                narrow_y(nbuf, 0, g).wait_recv()

            @pl.when(yb == 0)
            def _():
                narrow_y(gbuf, 1, g).wait_recv()

            block = nt(gbuf[g, g_own[g]], pair(nbuf, g))
            for b in range(2):
                of_s = slice(b * tok, (b + 1) * tok)
                keep = keep_of(k, b if z == 0 else 2 + b)
                kept = jnp.where(keep, block[:, of_s], 0.0).astype(bf16)
                for p in range(per_block):
                    term_n[p, i, :, of_s] = kept[p * rows : (p + 1) * rows]
        go_tn.start()

        def total(ref, count):
            out = ref[0].astype(f32)
            for i in range(1, count):
                out = out + ref[i].astype(f32)
            return out

        @pl.when(makes_w(t_own))
        def _():
            red_w[d] = term_w[slot_w(t_own) * per_block + part(d)]
            go_tw.arrive()
            dp_w[...] = total(red_w, dp_count).astype(bf16)
            span_w[my_span] = dp_w[...]

        go_sw.start()

        for i, g in enumerate(narrow):
            if z == 0:
                give_u(g, nn(own_rows(g, yb), pair(nbuf, g)))
            else:
                own_n = tn(own_cols(g, yb), pair(gbuf, g))
                give_back(g, own_n)
        for i, g in enumerate(narrow):
            pz_take = pz[i]
            pz_take.wait_recv()
            if z == 0:
                own_n = tn(own_cols(g, yb), pair(gbuf, g))
                give_back(g, recv_z[i].astype(f32) + own_n)
            else:
                give_u(g, recv_z[i].astype(f32) + nn(own_rows(g, yb), pair(nbuf, g)))

        @pl.when(makes_n(t_own))
        def _():
            red_n[d] = term_n[part(d)]
            go_tn.arrive()
            dp_n[...] = total(red_n, dp_count).astype(bf16)
            span_n[my_span] = dp_n[...]

        go_sn.start()

        @pl.when(makes_w(t_own))
        def _():
            go_sw.arrive()
            all_w[k] = total(span_w, spans).astype(bf16)

        go_aw.start()

        def send_vectors():
            gain_sum = jnp.sum(acc_gain[...], axis=0, keepdims=True)
            shift_sum = jnp.sum(acc_shift[...], axis=0, keepdims=True)
            for i in range(parts):
                vec_s[0, i : i + 1, :] = gain_sum[:, i * span : (i + 1) * span]
                vec_s[0, parts + i : parts + i + 1, :] = shift_sum[:, i * span : (i + 1) * span]
            go_va.start()
            vec_a[d] = vec_s[0]

        if z == 1:
            send_vectors()
            give_v()

        @pl.when(makes_n(t_own))
        def _():
            go_sn.arrive()
            all_n[k] = total(span_n, spans).astype(bf16)

        go_an.start()

        for i, g in enumerate(wide):
            py[i].wait_recv()
            whole = own_part[i] + recv_y[i].astype(f32)
            if z == 0:
                give_back(g, whole)
            else:
                give_u(g, whole)
        if z == 0:
            send_vectors()
            give_v()

        go_va.arrive()
        vec_s[1] = total(vec_a, dp_count)
        go_vb.start()
        vec_b[k] = vec_s[1]

        go_aw.arrive()
        go_an.arrive()

        def put(g, first, block):
            grad_mix[:, g, first * tok : first * tok + block.shape[1]] = block.astype(f32)

        for i in range(hg):
            put(i, 0, all_w[lax.rem(t_own, 2), i])

        @pl.when(t_own >= 2)
        def _():
            for i in range(hg):
                put(i, 2, all_n[t_own, i])
                for b in range(2):
                    put(hg + i, b, all_w[2 + b, i][:, :tok])
                    put(hg + i, b + 2, all_w[2 + b, i][:, tok:])

        @pl.when(t_own < 2)
        def _():
            for i in range(hg):
                put(hg + i, 0, all_n[t_own, i])

        go_vb.arrive()
        vec_s[2] = total(vec_b, QUAD)
        go_vc.start()
        vec_c[my_span] = vec_s[2]
        go_vc.arrive()
        summed[...] = total(vec_c, spans)

        for g in wide:
            y_send[g].wait_send()
        for g in narrow:
            z_send[g].wait_send()

            @pl.when(yb == 0)
            def _():
                narrow_y(nbuf, 0, g).wait_send()

            @pl.when(yb == 1)
            def _():
                narrow_y(gbuf, 1, g).wait_send()

        for i in range(hg):
            py[i].wait_send()
            pz[i].wait_send()
        for go in go_mix + [go_tw, go_tn, go_sw, go_sn, go_aw, go_an, go_va, go_vb, go_vc]:
            go.leave()

    for z in range(2):
        pl.when(zb == z)(functools.partial(run, z))


def finish(
    u_in, v_in, mix_in, summed, grad_u, grad_v, grad_mix, grad_bias, grad_gain, grad_shift, sems
):
    copies = [
        pltpu.make_async_copy(src, dst, sems.at[i])
        for i, (src, dst) in enumerate(((u_in, grad_u), (v_in, grad_v), (mix_in, grad_mix)))
    ]
    for copy in copies:
        copy.start()
    groups, span = grad_bias.shape
    parts = grad_gain.shape[-1] // span
    for i in range(parts):
        grad_gain[:, i * span : (i + 1) * span] = summed[i : i + 1, :]
        grad_shift[:, i * span : (i + 1) * span] = summed[parts + i : parts + i + 1, :]
    grad_bias[...] = summed[2 * parts : 2 * parts + groups, :]
    for copy in copies:
        copy.wait()


def per_device(gated, values_in, upstream, gain, shift, mix_w, mix_bias):
    dp_count = lax.axis_size("dp")
    sp_count = lax.axis_size("sp")
    tok, half = gated.shape[1:]
    rows, groups, span = mix_w.shape
    width = half // groups
    assert span == QUAD * tok and groups % 2 == 0 and tok % rows == 0
    spans = sp_count // QUAD
    hg = groups // 2
    vec_rows = 2 * (half // span) + groups
    f32, bf16 = jnp.float32, jnp.bfloat16
    hbm = pl.BlockSpec(memory_space=pltpu.HBM)
    vmem = pl.BlockSpec(memory_space=pltpu.VMEM)
    dma = pltpu.SemaphoreType.DMA
    term = (hg, rows, 2 * tok)
    scratch = (
        [pltpu.VMEM((tok, half), bf16)] * 3
        + [
            pltpu.VMEM((rows, groups, span), bf16),
            pltpu.VMEM((tok, half), f32),
            pltpu.VMEM((tok, 128), f32),
            pltpu.VMEM((groups, 2, tok, width), bf16),
            pltpu.VMEM((groups, 2, tok, width), bf16),
            pltpu.VMEM((groups, rows, 2 * tok), bf16),
            pltpu.VMEM((2 * (tok // rows), groups, rows, 2 * tok), bf16),
        ]
        + [pltpu.VMEM((hg, tok, width), bf16)] * 4
        + [
            pltpu.VMEM((hg, tok, width), f32),
            pltpu.VMEM((groups, tok, width), bf16),
            pltpu.VMEM((tok, 128), f32),
            pltpu.VMEM((tok, 128), f32),
            pltpu.VMEM((8, half), f32),
            pltpu.VMEM((8, half), f32),
            pltpu.VMEM((2 * (tok // rows),) + term, bf16),
            pltpu.VMEM((tok // rows,) + term, bf16),
            pltpu.VMEM((dp_count,) + term, bf16),
            pltpu.VMEM((dp_count,) + term, bf16),
            pltpu.VMEM(term, bf16),
            pltpu.VMEM(term, bf16),
            pltpu.VMEM((spans,) + term, bf16),
            pltpu.VMEM((spans,) + term, bf16),
            pltpu.VMEM((QUAD,) + term, bf16),
            pltpu.VMEM((QUAD,) + term, bf16),
            pltpu.VMEM((dp_count, vec_rows, span), f32),
            pltpu.VMEM((QUAD, vec_rows, span), f32),
            pltpu.VMEM((spans, vec_rows, span), f32),
            pltpu.VMEM((3, vec_rows, span), f32),
            pltpu.VMEM((groups, tok, 128), f32),
        ]
        + [dma((4, groups)), dma((4, hg))]
        + [dma((5, dp_count))] * 2
        + [dma((3, spans))] * 2
        + [dma((3, QUAD))] * 2
        + [dma((4,))]
    )
    out = pl.pallas_call(
        functools.partial(kernel, (tok, width, groups, span, dp_count, spans)),
        out_shape=(
            jax.ShapeDtypeStruct((tok, half), bf16),
            jax.ShapeDtypeStruct((tok, half), bf16),
            jax.ShapeDtypeStruct((rows, groups, span), f32),
            jax.ShapeDtypeStruct((vec_rows, span), f32),
        ),
        in_specs=[hbm] * 3 + [vmem] * 2 + [hbm, vmem],
        out_specs=[vmem] * 4,
        scratch_shapes=scratch,
        compiler_params=pltpu.CompilerParams(
            collective_id=0, has_side_effects=True, vmem_limit_bytes=60 * 1024 * 1024
        ),
    )(
        gated[0],
        values_in[0],
        upstream[0],
        gain[None],
        shift[None],
        mix_w,
        mix_bias,
    )
    u, v, mix, bias, gain_g, shift_g = pl.pallas_call(
        finish,
        out_shape=(
            jax.ShapeDtypeStruct((tok, half), bf16),
            jax.ShapeDtypeStruct((tok, half), bf16),
            jax.ShapeDtypeStruct((rows, groups, span), f32),
            jax.ShapeDtypeStruct((groups, span), f32),
            jax.ShapeDtypeStruct((1, half), f32),
            jax.ShapeDtypeStruct((1, half), f32),
        ),
        in_specs=[vmem] * 4,
        out_specs=[hbm] * 3 + [vmem] * 3,
        scratch_shapes=[pltpu.SemaphoreType.DMA((3,))],
        compiler_params=pltpu.CompilerParams(vmem_limit_bytes=60 * 1024 * 1024),
    )(*out)
    return (u[None], v[None], mix, bias, gain_g[0], shift_g[0])


def solution(mesh):
    placed = (
        P("dp", "sp", None),
        P("dp", "sp", None),
        P("dp", "sp", None),
        P(),
        P(),
        P("dp", None, None),
        P(),
    )
    return jax.shard_map(
        per_device,
        mesh=mesh,
        in_specs=placed,
        out_specs=(P("dp", "sp", None), P("dp", "sp", None), P("dp", None, None), P(), P(), P()),
        check_vma=False,
    )
```

```python
import functools

import jax
import jax.numpy as jnp
from jax import lax
from jax.experimental import pallas as pl
from jax.experimental.pallas import tpu as pltpu
from jax.sharding import PartitionSpec as P

SEG = 64

EPS = 1e-05

CHUNK = 16

QUAD = 4


def nt(a, b):
    return lax.dot_general(a, b, (((1,), (1,)), ((), ())), preferred_element_type=jnp.float32)


def tn(a, b):
    return lax.dot_general(a, b, (((0,), (0,)), ((), ())), preferred_element_type=jnp.float32)


def nn(a, b):
    return jnp.dot(a, b, preferred_element_type=jnp.float32)


def kernel(
    dims,
    gated_in,
    values_in,
    upstream_in,
    gain_in,
    shift_in,
    mix_in,
    bias_in,
    grad_u,
    grad_v,
    grad_mix,
    summed,
    gated,
    values,
    upstream,
    mix_w,
    gain,
    shift,
    mix_bias,
    unit,
    inv,
    nbuf,
    gbuf,
    w_send,
    w_block,
    stage_y,
    stage_z,
    recv_y,
    recv_z,
    own_part,
    back,
    sum_a,
    sum_b,
    acc_gain,
    acc_shift,
    term_w,
    term_d,
    term_l,
    red_w,
    red_d,
    red_l,
    dp_w,
    dp_d,
    dp_l,
    span_w,
    span_d,
    span_l,
    all_w,
    all_d,
    all_l,
    late_s,
    late_a,
    late_b,
    early_s,
    early_a,
    early_b,
    early_c,
    bias_t,
    raw_sems,
    part_sems,
    z_sems,
    dp_send,
    mix_recv,
    red_recv,
    vec_sems,
    sn_send,
    sn_recv,
    sq_send,
    sq_recv,
    in_sem,
):
    tok, width, groups, span, dp_count, spans = dims
    half = groups * width
    rows = span // dp_count
    per_block = tok // rows
    hg = groups // 2
    me = lax.axis_index("sp")
    my_span, k = me // QUAD, lax.rem(me, QUAD)
    zb, yb = k // 2, lax.rem(k, 2)
    d = lax.axis_index("dp")
    t_own = d // per_block
    f32, bf16 = jnp.float32, jnp.bfloat16

    def sq_id(j):
        return {"sp": my_span * QUAD + j}

    def dp_id(j):
        return {"dp": j}

    def sn_id(j):
        return {"sp": j * QUAD + k}

    def sp_id(j):
        return {"sp": j}

    y_id = sq_id(k + 1 - 2 * yb)
    z_id = sq_id(k + 2 - 4 * zb)

    def remote(src, dst, send, recv, where):
        return pltpu.make_async_remote_copy(
            src_ref=src,
            dst_ref=dst,
            send_sem=send,
            recv_sem=recv,
            device_id=where,
            device_id_type=pl.DeviceIdType.MESH,
        )

    class Exchange:
        def __init__(
            self, src, dst, own, count, where, send, recv, gives=None, takes=None, bulk=None
        ):
            self.src, self.dst, self.own, self.count = src, dst, own, count
            self.where, self.send, self.recv = where, send, recv
            self.gives, self.takes, self.bulk = gives, takes, bulk

        def copy(self, step, to):
            peer = lax.rem(self.own + step, self.count)
            landing = self.own if to else peer
            by = step if to else self.count - step
            return remote(
                self.src(peer) if to else self.dst(landing),
                self.dst(landing),
                self.send(step - 1),
                self.recv(by - 1),
                self.where(peer),
            )

        def each(self, cond, act):
            for step in range(1, self.count):
                if cond is None:
                    act(step)
                else:
                    pl.when(cond(lax.rem(self.own + step, self.count)))(lambda: act(step))

        def all_of_it(self):
            where = self.where(lax.rem(self.own + 1, self.count))
            return remote(self.bulk, self.bulk, self.send(0), self.recv(0), where)

        def start(self):
            self.each(self.gives, lambda step: self.copy(step, True).start())

        def arrive(self):
            if self.bulk is None:
                self.each(self.takes, lambda step: self.copy(step, False).wait_recv())
            elif self.takes is None:
                self.all_of_it().wait_recv()
            else:
                pl.when(self.takes(self.own))(lambda: self.all_of_it().wait_recv())

        def leave(self):
            if self.bulk is None or self.gives is not None:
                self.each(self.gives, lambda step: self.copy(step, True).wait_send())
            else:
                self.all_of_it().wait_send()

    def across(src, dst, send, recv, gives=None, takes=None, bulk=None):
        return Exchange(src, dst, d, dp_count, dp_id, send, recv, gives, takes, bulk)

    def spanning(src, dst, slot, gives=None, takes=None):
        return Exchange(
            src,
            dst,
            my_span,
            spans,
            sn_id,
            lambda step: sn_send.at[slot, step],
            lambda step: sn_recv.at[slot, step],
            gives,
            takes,
        )

    fetches = [
        pltpu.make_async_copy(src, dst, in_sem.at[i])
        for i, (src, dst) in enumerate(
            (
                (gated_in, gated),
                (upstream_in, upstream),
                (values_in, values),
                (mix_in, mix_w),
                (gain_in, gain),
                (shift_in, shift),
                (bias_in, mix_bias),
            )
        )
    ]
    for fetch in (*fetches[4:], fetches[2], fetches[0], fetches[1], fetches[3]):
        fetch.start()

    barrier = pltpu.get_barrier_semaphore()
    for own, count, where in ((me, spans * QUAD, sp_id), (d, dp_count, dp_id)):
        for step in range(1, count):
            pl.semaphore_signal(
                barrier,
                inc=1,
                device_id=where(lax.rem(own + step, count)),
                device_id_type=pl.DeviceIdType.MESH,
            )

    def piece(r):
        return pl.ds(pl.multiple_of(r * CHUNK, CHUNK), CHUNK)

    def lanes_of(g):
        return slice(g * width, (g + 1) * width)

    def allowed(first_t, first_s, n_t, n_s):
        t = first_t + lax.broadcasted_iota(jnp.int32, (n_t, n_s), 0)
        s = first_s + lax.broadcasted_iota(jnp.int32, (n_t, n_s), 1)
        return lax.div(t, SEG) >= lax.div(s, SEG)

    def run(z):
        first = range(hg)
        second = range(hg, groups)
        wide = first if z == 0 else second
        narrow = second if z == 0 else first
        n_own = {g: yb if (z == 0 or g in first) else 1 for g in range(groups)}
        g_own = {g: yb if (z == 1 or g in second) else 0 for g in range(groups)}

        def makes_w(t):
            return (lax.rem(t, 2) == yb) if z == 0 else (t >= 2)

        def slot_w(t):
            return lax.div(t, 2) if z == 0 else t - 2

        def makes_n(t):
            return t == k

        def of(j):
            return j // per_block

        def part(j):
            return lax.rem(j, per_block)

        x_buf = nbuf if z == 0 else gbuf
        o_buf = gbuf if z == 0 else nbuf
        raw_y = {}
        for g in wide:
            raw_y[g] = x_buf
        y_send = {
            g: remote(
                x_buf.at[g, yb], x_buf.at[g, yb], raw_sems.at[0, g], raw_sems.at[1, g], y_id
            )
            for g in wide
        }
        y_take = {
            g: remote(
                x_buf.at[g, 1 - yb],
                x_buf.at[g, 1 - yb],
                raw_sems.at[0, g],
                raw_sems.at[1, g],
                y_id,
            )
            for g in wide
        }

        def narrow_y(buf, slot, g):
            return remote(
                buf.at[g, slot], buf.at[g, slot], raw_sems.at[0, g], raw_sems.at[1, g], y_id
            )

        z_buf = nbuf if z == 0 else gbuf
        z_own = n_own if z == 0 else g_own
        z_slot = 0 if z == 0 else 1
        z_send = {
            g: remote(
                z_buf.at[g, z_own[g]],
                z_buf.at[g, z_slot],
                z_sems.at[0, i],
                z_sems.at[1, i],
                z_id,
            )
            for i, g in enumerate(narrow)
        }
        z_take = {
            g: remote(
                o_buf.at[g, 1 - z_slot],
                o_buf.at[g, 1 - z_slot],
                z_sems.at[0, i],
                z_sems.at[1, i],
                z_id,
            )
            for i, g in enumerate(wide)
        }
        py = [
            remote(stage_y.at[i], recv_y.at[i], part_sems.at[0, i], part_sems.at[1, i], y_id)
            for i in range(hg)
        ]
        pz = [
            remote(stage_z.at[i], recv_z.at[i], part_sems.at[2, i], part_sems.at[3, i], z_id)
            for i in range(hg)
        ]

        def needs(h):
            return makes_w if h == z else ((lambda t: t < 2) if z == 0 else (lambda t: t >= 2))

        def slot_of(h, t):
            return slot_w(t) if h == z else (t if z == 0 else t - 2)

        def w_at(h, j):
            return w_block.at[slot_of(h, of(j)) * per_block + part(j), h * hg : (h + 1) * hg]

        go_mix = [
            across(
                lambda j, h=h: w_send.at[h * hg : (h + 1) * hg],
                lambda j, h=h: w_at(h, j),
                lambda step, h=h: dp_send.at[h, step],
                lambda step, h=h: mix_recv.at[h, step],
                lambda j, h=h: needs(h)(t_own),
                lambda j, h=h: needs(h)(of(j)),
            )
            for h in range(2)
        ]
        def makes_l(t):
            return (t == k) & (yb == 1)

        def peer_w(j):
            return ((j < 2) & (lax.rem(t_own, 2) == j)) | ((j >= 2) & (t_own >= 2))

        def peer_d(j):
            return t_own == j

        def peer_l(j):
            return (t_own == j) & (lax.rem(j, 2) == 1)

        class Reduction:
            def __init__(self, makes, peer, source, refs, slot):
                red, dp_sum, over, every, bulk = refs
                self.makes, self.refs, self.source = makes, refs, source
                self.to_dp = across(
                    source,
                    lambda j: red(j),
                    lambda step: dp_send.at[2 + slot, step],
                    lambda step: red_recv.at[slot],
                    lambda j: makes(of(j)),
                    lambda j: makes(t_own),
                    bulk,
                )
                self.to_span = spanning(
                    lambda j: dp_sum,
                    lambda j: over(j),
                    slot,
                    lambda j: makes(t_own),
                    lambda j: makes(t_own),
                )
                self.peer = peer
                row, column = k + 1 - 2 * yb, k + 2 - 4 * zb

                def copy(piece, at, where):
                    return remote(
                        every(piece),
                        every(piece),
                        sq_send.at[slot, at],
                        sq_recv.at[slot, at],
                        where,
                    )

                self.own_z, self.own_y = copy(k, 0, z_id), copy(k, 1, y_id)
                self.take_z, self.take_y = copy(column, 0, z_id), copy(row, 1, y_id)
                self.relay_z = copy(row, 2, z_id)
                self.take_relay = copy(3 - k, 2, z_id)
                self.row, self.column = row, column

            def start(self):
                self.to_dp.start()

            def over_spans(self):
                red, dp_sum, over, every, _bulk = self.refs

                @pl.when(self.makes(t_own))
                def _():
                    red(d)[...] = self.source(d)[...]
                    self.to_dp.arrive()
                    dp_sum[...] = total(red, dp_count).astype(bf16)
                    self.to_span.start()
                    over(my_span)[...] = dp_sum[...]

            def pass_round(self):
                red, dp_sum, over, every, _bulk = self.refs

                @pl.when(self.makes(t_own))
                def _():
                    self.to_span.arrive()
                    every(k)[...] = total(over, spans).astype(bf16)
                    self.own_z.start()
                    self.own_y.start()

            def relay(self):
                @pl.when(self.peer(self.row))
                def _():
                    self.take_y.wait_recv()
                    self.relay_z.start()

            def arrive(self):
                pl.when(self.peer(self.column))(lambda: self.take_z.wait_recv())
                pl.when(self.peer(3 - k))(lambda: self.take_relay.wait_recv())

            def leave(self):
                self.to_dp.leave()
                self.to_span.leave()

                @pl.when(self.makes(t_own))
                def _():
                    self.own_z.wait_send()
                    self.own_y.wait_send()

                pl.when(self.peer(self.row))(lambda: self.relay_z.wait_send())

        def total(at, count):
            out = at(0)[...].astype(f32)
            for i in range(1, count):
                out = out + at(i)[...].astype(f32)
            return out

        terms_w = [
            Reduction(
                makes_w,
                peer_w,
                lambda j, i=i: term_w.at[slot_w(of(j)) * per_block + part(j), i],
                (
                    lambda j, i=i: red_w.at[i, j],
                    dp_w.at[i],
                    lambda j, i=i: span_w.at[j, i],
                    lambda j, i=i: all_w.at[j, i],
                    red_w.at[i, : dp_count - 1],
                ),
                i,
            )
            for i in range(hg)
        ]
        terms_d = Reduction(
            makes_n,
            peer_d,
            lambda j: term_d.at[part(j)],
            (
                lambda j: red_d.at[j],
                dp_d,
                lambda j: span_d.at[j],
                lambda j: all_d.at[j],
                red_d.at[: dp_count - 1],
            ),
            hg,
        )
        terms_l = Reduction(
            makes_l,
            peer_l,
            lambda j: term_l.at[part(j)],
            (
                lambda j: red_l.at[j],
                dp_l,
                lambda j: span_l.at[j],
                lambda j: all_l.at[j],
                red_l.at[: dp_count - 1],
            ),
            hg + 1,
        )

        def vec(at):
            return lambda step: vec_sems.at[at]

        late_go = (
            across(
                lambda j: late_s.at[0],
                lambda j: late_a.at[j],
                vec(0),
                vec(1),
                bulk=late_a.at[: dp_count - 1],
            ),
            Exchange(
                lambda j: late_s.at[1],
                lambda j: late_b.at[j],
                me,
                spans * QUAD,
                sp_id,
                vec(2),
                vec(3),
                bulk=late_b.at[: spans * QUAD - 1],
            ),
        )
        early_go = (
            across(
                lambda j: early_s.at[0],
                lambda j: early_a.at[j],
                vec(4),
                vec(5),
                bulk=early_a.at[: dp_count - 1],
            ),
            Exchange(
                lambda j: early_s.at[1],
                lambda j: early_c.at[j],
                me // 2,
                spans * QUAD // 2,
                lambda j: {"sp": 2 * j + lax.rem(me, 2)},
                vec(6),
                vec(7),
                bulk=early_c.at[: spans * QUAD // 2 - 1],
            ),
            Exchange(
                lambda j: early_s.at[2],
                lambda j: early_b.at[j],
                lax.rem(me, 2),
                2,
                lambda j: {"sp": me - lax.rem(me, 2) + j},
                vec(8),
                vec(9),
            ),
        )

        def make_normed():
            for fetch in (fetches[4], fetches[5], fetches[2]):
                fetch.wait()

            @pl.loop(0, tok // CHUNK, unroll=4)
            def _(r):
                at = piece(r)
                raw = values[at, :].astype(f32)
                centred = raw - jnp.mean(raw, axis=-1, keepdims=True)
                inv_std = lax.rsqrt(jnp.mean(centred * centred, axis=-1, keepdims=True) + EPS)
                one = centred * inv_std
                unit[at, :] = one
                inv[at, :] = jnp.broadcast_to(inv_std, (CHUNK, 128))
                normed = (one * gain[...] + shift[...]).astype(bf16)
                for g in range(groups):
                    nbuf[g, n_own[g], at, :] = normed[:, lanes_of(g)]

        def make_cotangent():
            fetches[0].wait()
            fetches[1].wait()

            @pl.loop(0, tok // CHUNK)
            def _(r):
                at = piece(r)
                prod = (upstream[at, :].astype(f32) * gated[at, :].astype(f32)).astype(bf16)
                for g in range(groups):
                    gbuf[g, g_own[g], at, :] = prod[:, lanes_of(g)]

        def meet():
            pl.semaphore_wait(barrier, spans * QUAD + dp_count - 2)

        def narrow_n():
            @pl.when(yb == 0)
            def _():
                for g in narrow:
                    narrow_y(nbuf, 0, g).start()

        def narrow_g():
            @pl.when(yb == 1)
            def _():
                for g in narrow:
                    narrow_y(gbuf, 1, g).start()

        (make_normed if z == 0 else make_cotangent)()
        meet()
        for g, h in zip(wide, narrow):
            y_send[g].start()
            z_send[h].start()
        (narrow_n if z == 0 else narrow_g)()
        (make_cotangent if z == 0 else make_normed)()
        (narrow_g if z == 0 else narrow_n)()

        @pl.when(yb == 0)
        def _():
            for g in narrow:
                nbuf[g, 1] = jnp.zeros((tok, width), bf16)

        @pl.when(yb == 1)
        def _():
            for g in narrow:
                gbuf[g, 0] = jnp.zeros((tok, width), bf16)

        fetches[3].wait()

        @pl.loop(0, rows // CHUNK)
        def _(r):
            at = piece(r)
            for c in range(2):
                for h in range(2):
                    if z == 0:
                        col = c
                    elif h == 0:
                        col = 2 + c
                    else:
                        col = yb + 2 * c
                    start = col * tok
                    if not isinstance(start, int):
                        start = pl.multiple_of(start, tok)
                    block = mix_w[at, :, pl.ds(start, tok)].astype(f32)
                    keep = allowed(d * rows + r * CHUNK, col * tok, CHUNK, tok)
                    for g in range(h * hg, (h + 1) * hg):
                        w_send[g, at, c * tok : (c + 1) * tok] = jnp.where(
                            keep, block[:, g, :], 0.0
                        ).astype(bf16)

        for h in (z, 1 - z):
            go_mix[h].start()

            @pl.when(needs(h)(t_own))
            def _():
                w_at(h, d)[...] = w_send[h * hg : (h + 1) * hg]

        for i, g in enumerate(narrow):
            block = nt(gbuf[g, g_own[g]], nbuf[g, n_own[g]])
            kept = jnp.where(allowed(0, 0, tok, tok), block, 0.0).astype(bf16)
            for p in range(per_block):
                term_d[p, i] = kept[p * rows : (p + 1) * rows]
        terms_d.start()

        fetches[6].wait()
        own_bias = mix_bias[:, 0:tok]
        for b in range(1, QUAD):
            own_bias = jnp.where(k == b, mix_bias[:, b * tok : (b + 1) * tok], own_bias)
        for g in range(groups):
            bias_t[g] = jnp.transpose(jnp.broadcast_to(own_bias[g : g + 1], (128, tok)))
        acc_gain[...] = jnp.zeros_like(acc_gain)
        acc_shift[...] = jnp.zeros_like(acc_shift)
        sum_a[...] = jnp.zeros_like(sum_a)
        sum_b[...] = jnp.zeros_like(sum_b)
        grad_mix[...] = jnp.zeros_like(grad_mix)
        lines = hg * width // 128
        per_span = span // 128
        for g in range(groups):
            bias_sum = nt(jnp.ones((8, width), bf16), gbuf[g, g_own[g]])[0:1]
            for b in range(QUAD):
                shown = jnp.where(k == b, bias_sum, 0.0)
                for c in range(tok // 128):
                    at = 2 * lines + g * per_span + b * (tok // 128) + c
                    early_s[0, at : at + 1, :] = shown[:, c * 128 : (c + 1) * 128]

        def give_u(g, mixed):
            for c in range(width // 128):
                lanes = slice(c * 128, (c + 1) * 128)
                at = slice(g * width + c * 128, g * width + (c + 1) * 128)
                whole = (mixed[:, lanes] + bias_t[g]).astype(bf16).astype(f32)
                grad_u[:, at] = (upstream[:, at].astype(f32) * whole).astype(bf16)

        def give_back(g, total):
            back[g] = total.astype(bf16)

            @pl.loop(0, tok // CHUNK)
            def _(r):
                at = piece(r)
                grad_normed = back[g, at, :].astype(f32)
                one = unit[at, lanes_of(g)]
                prod = grad_normed * one
                acc_gain[:, lanes_of(g)] += prod[0:8] + prod[8:16]
                acc_shift[:, lanes_of(g)] += grad_normed[0:8] + grad_normed[8:16]
                scaled = grad_normed * gain[:, lanes_of(g)]
                prod = scaled * one
                a, b = scaled[:, 0:128], prod[:, 0:128]
                for c in range(1, width // 128):
                    a = a + scaled[:, c * 128 : (c + 1) * 128]
                    b = b + prod[:, c * 128 : (c + 1) * 128]
                sum_a[at, :] += a
                sum_b[at, :] += b

        def give_v():
            @pl.loop(0, tok // CHUNK)
            def _(r):
                at = piece(r)
                mean_a = jnp.sum(sum_a[at, :], axis=-1, keepdims=True) / half
                mean_b = jnp.sum(sum_b[at, :], axis=-1, keepdims=True) / half
                inv_std = inv[at, :][:, 0:1]
                for g in range(groups):
                    scaled = back[g, at, :].astype(f32) * gain[:, lanes_of(g)]
                    grad_v[at, lanes_of(g)] = (
                        inv_std * (scaled - mean_a - unit[at, lanes_of(g)] * mean_b)
                    ).astype(bf16)

        def own_cols(g, block):
            at = pl.ds(pl.multiple_of(block * tok, tok), tok)
            return w_block[:, g, :, at].reshape(2 * tok, tok)

        def own_rows(g, block):
            return w_block[pl.ds(block * per_block, per_block), g].reshape(tok, 2 * tok)

        def pair(buf, g):
            return buf[g].reshape(2 * tok, width)

        def keep_of(row, col):
            return allowed(row * tok, col * tok, tok, tok)

        def gather_sums(h, out):
            first = h * hg * width
            for ref, line in ((acc_gain, 0), (acc_shift, lines)):
                whole = jnp.sum(ref[:, first : first + hg * width], axis=0, keepdims=True)
                for i in range(lines):
                    out[0, line + i : line + i + 1, :] = whole[:, i * 128 : (i + 1) * 128]

        def send_early():
            gather_sums(1, early_s)
            early_go[0].start()
            early_a[d] = early_s[0]

        def spread_early():
            early_go[0].arrive()
            early_s[1] = total(lambda j: early_a.at[j], dp_count)
            early_go[1].start()
            early_c[me // 2] = early_s[1]

        def respread_early():
            early_go[1].arrive()
            early_s[2] = total(lambda j: early_c.at[j], spans * QUAD // 2)
            early_go[2].start()
            early_b[lax.rem(me, 2)] = early_s[2]

        def send_late():
            gather_sums(0, late_s)
            late_go[0].start()
            late_a[d] = late_s[0]

        def spread_late():
            late_go[0].arrive()
            late_s[1] = total(lambda j: late_a.at[j], dp_count)
            late_go[1].start()
            late_b[me] = late_s[1]

        def take_early():
            early_go[2].arrive()
            summed[2 * lines :, :] = total(lambda j: early_b.at[j], 2)

        def take_late():
            late_go[1].arrive()
            summed[: 2 * lines, :] = total(lambda j: late_b.at[j], spans * QUAD)

        go_mix[z].arrive()
        for i, g in enumerate(wide):
            y_take[g].wait_recv()
            if z == 0:
                both = nn(w_block[:, g].reshape(2 * tok, 2 * tok), pair(nbuf, g))
                stage_z[i] = both[tok:].astype(bf16)
                pz[i].start()
                give_u(g, both[:tok])
            else:
                both = tn(w_block[:, g].reshape(2 * tok, 2 * tok), pair(gbuf, g))
                stage_z[i] = both[:tok].astype(bf16)
                pz[i].start()
                give_back(g, both[tok:])
            z_take[g].wait_recv()
            if z == 0:
                stage_y[i] = tn(own_cols(g, 1 - yb), pair(gbuf, g)).astype(bf16)
            else:
                stage_y[i] = nn(own_rows(g, 1 - yb), pair(nbuf, g)).astype(bf16)
            if z == 0 or i < hg - 1:
                py[i].start()
            block = nt(pair(gbuf, g), pair(nbuf, g))
            for a in range(2):
                for b in range(2):
                    if z == 0:
                        keep = keep_of(yb + 2 * a, b)
                    else:
                        keep = keep_of(2 + a, yb + 2 * b)
                    at, of_s = slice(a * tok, (a + 1) * tok), slice(b * tok, (b + 1) * tok)
                    kept = jnp.where(keep, block[at, of_s], 0.0).astype(bf16)
                    for p in range(per_block):
                        term_w[a * per_block + p, i, :, of_s] = kept[p * rows : (p + 1) * rows]
            terms_w[i].start()
            if z == 0:
                own_part[i] = tn(own_cols(g, yb), pair(gbuf, g))
            else:
                own_part[i] = nn(own_rows(g, yb), pair(nbuf, g))

        go_mix[1 - z].arrive()
        terms_d.over_spans()
        for i, g in enumerate(narrow):
            terms_w[i].over_spans()

            @pl.when(yb == 1)
            def _():
                narrow_y(nbuf, 0, g).wait_recv()
                block = nt(gbuf[g, g_own[g]], nbuf[g, 0]).astype(bf16)
                for p in range(per_block):
                    term_l[p, i] = block[p * rows : (p + 1) * rows]

            @pl.when(yb == 0)
            def _():
                narrow_y(gbuf, 1, g).wait_recv()

            if i == hg - 1:
                terms_l.start()
            if z == 0:
                give_u(g, nn(own_rows(g, yb), pair(nbuf, g)))
            pz[i].wait_recv()
            if z == 0:
                give_back(g, recv_z[i].astype(f32) + tn(own_cols(g, yb), pair(gbuf, g)))
            else:
                give_back(g, tn(own_cols(g, yb), pair(gbuf, g)))
                give_u(g, recv_z[i].astype(f32) + nn(own_rows(g, yb), pair(nbuf, g)))

        send_early()
        if z == 1:
            send_late()
        terms_d.pass_round()
        for term in terms_w:
            term.pass_round()
        if z == 1:
            py[hg - 1].start()
        if z == 1:
            give_v()
        spread_early()
        if z == 1:
            spread_late()
        terms_l.over_spans()

        def relay_terms():
            for term in (terms_d, *terms_w):
                term.relay()

        for i, g in enumerate(wide):
            if z == 1 and i == hg - 1:
                relay_terms()
                respread_early()
                terms_l.pass_round()
            py[i].wait_recv()
            whole = own_part[i] + recv_y[i].astype(f32)
            if z == 0:
                give_back(g, whole)
            else:
                give_u(g, whole)
        if z == 0:
            send_late()
            respread_early()
            spread_late()
            terms_l.pass_round()
            relay_terms()
            give_v()

        def put(g, first, block):
            grad_mix[:, g, first * tok : first * tok + block.shape[1]] = block.astype(f32)

        for g in wide:
            y_send[g].wait_send()
        for g in narrow:
            z_send[g].wait_send()

            @pl.when(yb == 0)
            def _():
                narrow_y(nbuf, 0, g).wait_send()

            @pl.when(yb == 1)
            def _():
                narrow_y(gbuf, 1, g).wait_send()

        for i in range(hg):
            py[i].wait_send()
            pz[i].wait_send()
        for go in (*go_mix, late_go[0], early_go[0]):
            go.leave()

        terms_d.arrive()
        for t in range(QUAD):

            @pl.when(t_own == t)
            def _():
                for i in range(hg):
                    put(i if t >= 2 else hg + i, t, all_d[t, i])

        terms_d.leave()
        for i, term in enumerate(terms_w):
            term.arrive()
            put(i, 0, all_w[lax.rem(t_own, 2), i])

            @pl.when(t_own >= 2)
            def _():
                for b in range(2):
                    put(hg + i, b, all_w[2 + b, i][:, :tok])

            for t in range(2, QUAD):

                @pl.when(t_own == t)
                def _():
                    for b in range(t - 1):
                        put(hg + i, b + 2, all_w[2 + b, i][:, tok:])

            term.leave()
        terms_l.relay()
        terms_l.arrive()
        for t in range(1, QUAD, 2):

            @pl.when(t_own == t)
            def _():
                for i in range(hg):
                    put(i if t >= 2 else hg + i, t - 1, all_l[t, i])

        terms_l.leave()
        take_early()
        for go in early_go[1:]:
            go.leave()
        take_late()
        late_go[1].leave()

    for z in range(2):
        pl.when(zb == z)(functools.partial(run, z))


def finish(
    u_in, v_in, mix_in, summed, grad_u, grad_v, grad_mix, grad_bias, grad_gain, grad_shift, sems
):
    copies = [
        pltpu.make_async_copy(src, dst, sems.at[i])
        for i, (src, dst) in enumerate(((u_in, grad_u), (v_in, grad_v), (mix_in, grad_mix)))
    ]
    for copy in copies:
        copy.start()
    groups, span = grad_bias.shape
    lines = grad_gain.shape[-1] // 2 // 128
    per_span = span // 128
    for h in range(2):
        for i in range(lines):
            to = slice((h * lines + i) * 128, (h * lines + i + 1) * 128)
            at = 2 * h * lines + i
            grad_gain[:, to] = summed[at : at + 1, :]
            grad_shift[:, to] = summed[lines + at : lines + at + 1, :]
    for g in range(groups):
        for c in range(per_span):
            at = 4 * lines + g * per_span + c
            grad_bias[g : g + 1, c * 128 : (c + 1) * 128] = summed[at : at + 1, :]
    for copy in copies:
        copy.wait()


def per_device(gated, values_in, upstream, gain, shift, mix_w, mix_bias):
    dp_count = lax.axis_size("dp")
    sp_count = lax.axis_size("sp")
    tok, half = gated.shape[1:]
    rows, groups, span = mix_w.shape
    width = half // groups
    assert span == QUAD * tok and groups % 2 == 0 and tok % rows == 0
    spans = sp_count // QUAD
    hg = groups // 2
    f32, bf16 = jnp.float32, jnp.bfloat16
    hbm = pl.BlockSpec(memory_space=pltpu.HBM)
    vmem = pl.BlockSpec(memory_space=pltpu.VMEM)
    dma = pltpu.SemaphoreType.DMA
    term, slim = (hg, rows, 2 * tok), (hg, rows, tok)
    late_rows = half // 128
    early_rows = late_rows + groups * span // 128
    assert half % 256 == 0 and tok % 128 == 0
    scratch = (
        [pltpu.VMEM((tok, half), bf16)] * 3
        + [
            pltpu.VMEM((rows, groups, span), bf16),
            pltpu.VMEM((1, half), f32),
            pltpu.VMEM((1, half), f32),
            pltpu.VMEM((groups, span), f32),
            pltpu.VMEM((tok, half), f32),
            pltpu.VMEM((tok, 128), f32),
            pltpu.VMEM((groups, 2, tok, width), bf16),
            pltpu.VMEM((groups, 2, tok, width), bf16),
            pltpu.VMEM((groups, rows, 2 * tok), bf16),
            pltpu.VMEM((2 * (tok // rows), groups, rows, 2 * tok), bf16),
        ]
        + [pltpu.VMEM((hg, tok, width), bf16)] * 4
        + [
            pltpu.VMEM((hg, tok, width), f32),
            pltpu.VMEM((groups, tok, width), bf16),
            pltpu.VMEM((tok, 128), f32),
            pltpu.VMEM((tok, 128), f32),
            pltpu.VMEM((8, half), f32),
            pltpu.VMEM((8, half), f32),
            pltpu.VMEM((2 * (tok // rows),) + term, bf16),
            pltpu.VMEM((tok // rows,) + slim, bf16),
            pltpu.VMEM((tok // rows,) + slim, bf16),
        ]
        + [pltpu.VMEM((hg, dp_count, rows, 2 * tok), bf16)]
        + [pltpu.VMEM((dp_count,) + shape, bf16) for shape in (slim, slim)]
        + [pltpu.VMEM(shape, bf16) for shape in (term, slim, slim)]
        + [pltpu.VMEM((spans,) + shape, bf16) for shape in (term, slim, slim)]
        + [pltpu.VMEM((QUAD,) + shape, bf16) for shape in (term, slim, slim)]
        + [
            pltpu.VMEM((2, late_rows, 128), f32),
            pltpu.VMEM((dp_count, late_rows, 128), f32),
            pltpu.VMEM((sp_count, late_rows, 128), f32),
            pltpu.VMEM((3, early_rows, 128), f32),
            pltpu.VMEM((dp_count, early_rows, 128), f32),
            pltpu.VMEM((2, early_rows, 128), f32),
            pltpu.VMEM((sp_count // 2, early_rows, 128), f32),
            pltpu.VMEM((groups, tok, 128), f32),
        ]
        + [dma((2, groups)), dma((4, hg)), dma((2, hg))]
        + [dma((4 + hg, dp_count - 1)), dma((2, dp_count - 1)), dma((2 + hg,)), dma((10,))]
        + [dma((2 + hg, spans - 1))] * 2
        + [dma((2 + hg, 3))] * 2
        + [dma((7,))]
    )
    out = pl.pallas_call(
        functools.partial(kernel, (tok, width, groups, span, dp_count, spans)),
        out_shape=(
            jax.ShapeDtypeStruct((tok, half), bf16),
            jax.ShapeDtypeStruct((tok, half), bf16),
            jax.ShapeDtypeStruct((rows, groups, span), f32),
            jax.ShapeDtypeStruct((late_rows + early_rows, 128), f32),
        ),
        in_specs=[hbm] * 7,
        out_specs=[vmem] * 4,
        scratch_shapes=scratch,
        compiler_params=pltpu.CompilerParams(
            collective_id=0, has_side_effects=True, vmem_limit_bytes=36 * 1024 * 1024
        ),
    )(
        *(
            pltpu.with_memory_space_constraint(x, pltpu.HBM)
            for x in (
                gated[0],
                values_in[0],
                upstream[0],
                gain[None],
                shift[None],
                mix_w,
                mix_bias,
            )
        )
    )
    u, v, mix, bias, gain_g, shift_g = pl.pallas_call(
        finish,
        out_shape=(
            jax.ShapeDtypeStruct((tok, half), bf16),
            jax.ShapeDtypeStruct((tok, half), bf16),
            jax.ShapeDtypeStruct((rows, groups, span), f32),
            jax.ShapeDtypeStruct((groups, span), f32),
            jax.ShapeDtypeStruct((1, half), f32),
            jax.ShapeDtypeStruct((1, half), f32),
        ),
        in_specs=[vmem] * 4,
        out_specs=[hbm] * 3 + [vmem] * 3,
        scratch_shapes=[pltpu.SemaphoreType.DMA((3,))],
        compiler_params=pltpu.CompilerParams(vmem_limit_bytes=36 * 1024 * 1024),
    )(*out)
    return (u[None], v[None], mix, bias, gain_g[0], shift_g[0])


def solution(mesh):
    placed = (
        P("dp", "sp", None),
        P("dp", "sp", None),
        P("dp", "sp", None),
        P(),
        P(),
        P("dp", None, None),
        P(),
    )
    return jax.shard_map(
        per_device,
        mesh=mesh,
        in_specs=placed,
        out_specs=(P("dp", "sp", None), P("dp", "sp", None), P("dp", None, None), P(), P(), P()),
        check_vma=False,
    )
```

```python
import functools

import jax
import jax.numpy as jnp
from jax import lax
from jax.experimental import pallas as pl
from jax.experimental.pallas import tpu as pltpu
from jax.sharding import PartitionSpec as P

SEG = 64

EPS = 1e-05

CHUNK = 16

QUAD = 4


def nt(a, b):
    return lax.dot_general(a, b, (((1,), (1,)), ((), ())), preferred_element_type=jnp.float32)


def tn(a, b):
    return lax.dot_general(a, b, (((0,), (0,)), ((), ())), preferred_element_type=jnp.float32)


def nn(a, b):
    return jnp.dot(a, b, preferred_element_type=jnp.float32)


def kernel(
    dims,
    gated_in,
    values_in,
    upstream_in,
    gain_in,
    shift_in,
    mix_in,
    bias_in,
    grad_u,
    grad_v,
    grad_mix,
    grad_gain,
    grad_shift,
    grad_bias,
    gated,
    values,
    upstream,
    mix_w,
    gain,
    shift,
    mix_bias,
    unit,
    inv,
    nbuf,
    gbuf,
    w_send,
    w_block,
    stage_y,
    stage_z,
    recv_y,
    recv_z,
    own_part,
    back,
    sum_a,
    sum_b,
    acc_gain,
    acc_shift,
    term_w,
    term_d,
    term_l,
    red_w,
    red_d,
    red_l,
    dp_w,
    dp_d,
    dp_l,
    span_w,
    span_d,
    span_l,
    all_w,
    all_d,
    all_l,
    late_s,
    late_a,
    late_b,
    early_s,
    early_a,
    early_b,
    early_c,
    bias_t,
    raw_sems,
    part_sems,
    z_sems,
    dp_send,
    mix_recv,
    red_recv,
    vec_sems,
    sn_send,
    sn_recv,
    sq_send,
    sq_recv,
    in_sem,
):
    tok, width, groups, span, dp_count, spans = dims
    half = groups * width
    rows = span // dp_count
    per_block = tok // rows
    hg = groups // 2
    me = lax.axis_index("sp")
    my_span, k = me // QUAD, lax.rem(me, QUAD)
    zb, yb = k // 2, lax.rem(k, 2)
    d = lax.axis_index("dp")
    t_own = d // per_block
    f32, bf16 = jnp.float32, jnp.bfloat16

    def sq_id(j):
        return {"sp": my_span * QUAD + j}

    def dp_id(j):
        return {"dp": j}

    def sn_id(j):
        return {"sp": j * QUAD + k}

    def sp_id(j):
        return {"sp": j}

    y_id = sq_id(k + 1 - 2 * yb)
    z_id = sq_id(k + 2 - 4 * zb)

    def remote(src, dst, send, recv, where):
        return pltpu.make_async_remote_copy(
            src_ref=src,
            dst_ref=dst,
            send_sem=send,
            recv_sem=recv,
            device_id=where,
            device_id_type=pl.DeviceIdType.MESH,
        )

    class Exchange:
        def __init__(
            self, src, dst, own, count, where, send, recv, gives=None, takes=None, bulk=None
        ):
            self.src, self.dst, self.own, self.count = src, dst, own, count
            self.where, self.send, self.recv = where, send, recv
            self.gives, self.takes, self.bulk = gives, takes, bulk

        def copy(self, step, to):
            peer = lax.rem(self.own + step, self.count)
            landing = self.own if to else peer
            by = step if to else self.count - step
            return remote(
                self.src(peer) if to else self.dst(landing),
                self.dst(landing),
                self.send(step - 1),
                self.recv(by - 1),
                self.where(peer),
            )

        def each(self, cond, act):
            for step in range(1, self.count):
                if cond is None:
                    act(step)
                else:
                    pl.when(cond(lax.rem(self.own + step, self.count)))(lambda: act(step))

        def all_of_it(self):
            where = self.where(lax.rem(self.own + 1, self.count))
            return remote(self.bulk, self.bulk, self.send(0), self.recv(0), where)

        def start(self):
            self.each(self.gives, lambda step: self.copy(step, True).start())

        def arrive(self):
            if self.bulk is None:
                self.each(self.takes, lambda step: self.copy(step, False).wait_recv())
            elif self.takes is None:
                self.all_of_it().wait_recv()
            else:
                pl.when(self.takes(self.own))(lambda: self.all_of_it().wait_recv())

        def leave(self):
            if self.bulk is None or self.gives is not None:
                self.each(self.gives, lambda step: self.copy(step, True).wait_send())
            else:
                self.all_of_it().wait_send()

    def across(src, dst, send, recv, gives=None, takes=None, bulk=None):
        return Exchange(src, dst, d, dp_count, dp_id, send, recv, gives, takes, bulk)

    def spanning(src, dst, slot, gives=None, takes=None):
        return Exchange(
            src,
            dst,
            my_span,
            spans,
            sn_id,
            lambda step: sn_send.at[slot, step],
            lambda step: sn_recv.at[slot, step],
            gives,
            takes,
        )

    fetches = [
        pltpu.make_async_copy(src, dst, in_sem.at[i])
        for i, (src, dst) in enumerate(
            (
                (gated_in, gated),
                (upstream_in, upstream),
                (values_in, values),
                (mix_in, mix_w),
                (gain_in, gain),
                (shift_in, shift),
                (bias_in, mix_bias),
            )
        )
    ]
    for z, order in ((0, (4, 5, 2, 0, 1, 3, 6)), (1, (0, 1, 2, 4, 5, 3, 6))):

        @pl.when(zb == z)
        def _():
            for i in order:
                fetches[i].start()

    barrier = pltpu.get_barrier_semaphore()
    for own, count, where in ((me, spans * QUAD, sp_id), (d, dp_count, dp_id)):
        for step in range(1, count):
            pl.semaphore_signal(
                barrier,
                inc=1,
                device_id=where(lax.rem(own + step, count)),
                device_id_type=pl.DeviceIdType.MESH,
            )

    def piece(r):
        return pl.ds(pl.multiple_of(r * CHUNK, CHUNK), CHUNK)

    def lanes_of(g):
        return slice(g * width, (g + 1) * width)

    def allowed(first_t, first_s, n_t, n_s):
        t = first_t + lax.broadcasted_iota(jnp.int32, (n_t, n_s), 0)
        s = first_s + lax.broadcasted_iota(jnp.int32, (n_t, n_s), 1)
        return lax.div(t, SEG) >= lax.div(s, SEG)

    def run(z):
        first = range(hg)
        second = range(hg, groups)
        wide = first if z == 0 else second
        narrow = second if z == 0 else first
        n_own = {g: yb if (z == 0 or g in first) else 1 for g in range(groups)}
        g_own = {g: yb if (z == 1 or g in second) else 0 for g in range(groups)}

        def makes_w(t):
            return (lax.rem(t, 2) == yb) if z == 0 else (t >= 2)

        def slot_w(t):
            return lax.div(t, 2) if z == 0 else t - 2

        def makes_n(t):
            return t == k

        def of(j):
            return j // per_block

        def part(j):
            return lax.rem(j, per_block)

        x_buf = nbuf if z == 0 else gbuf
        o_buf = gbuf if z == 0 else nbuf
        raw_y = {}
        for g in wide:
            raw_y[g] = x_buf
        y_send = {
            g: remote(
                x_buf.at[g, yb], x_buf.at[g, yb], raw_sems.at[0, g], raw_sems.at[1, g], y_id
            )
            for g in wide
        }
        y_take = {
            g: remote(
                x_buf.at[g, 1 - yb],
                x_buf.at[g, 1 - yb],
                raw_sems.at[0, g],
                raw_sems.at[1, g],
                y_id,
            )
            for g in wide
        }

        def narrow_y(buf, slot, g):
            return remote(
                buf.at[g, slot], buf.at[g, slot], raw_sems.at[0, g], raw_sems.at[1, g], y_id
            )

        z_buf = nbuf if z == 0 else gbuf
        z_own = n_own if z == 0 else g_own
        z_slot = 0 if z == 0 else 1
        z_send = {
            g: remote(
                z_buf.at[g, z_own[g]],
                z_buf.at[g, z_slot],
                z_sems.at[0, i],
                z_sems.at[1, i],
                z_id,
            )
            for i, g in enumerate(narrow)
        }
        z_take = {
            g: remote(
                o_buf.at[g, 1 - z_slot],
                o_buf.at[g, 1 - z_slot],
                z_sems.at[0, i],
                z_sems.at[1, i],
                z_id,
            )
            for i, g in enumerate(wide)
        }
        py = [
            remote(stage_y.at[i], recv_y.at[i], part_sems.at[0, i], part_sems.at[1, i], y_id)
            for i in range(hg)
        ]
        pz = [
            remote(stage_z.at[i], recv_z.at[i], part_sems.at[2, i], part_sems.at[3, i], z_id)
            for i in range(hg)
        ]

        def needs(h):
            return makes_w if h == z else ((lambda t: t < 2) if z == 0 else (lambda t: t >= 2))

        def slot_of(h, t):
            return slot_w(t) if h == z else (t if z == 0 else t - 2)

        def w_at(h, j):
            return w_block.at[slot_of(h, of(j)) * per_block + part(j), h * hg : (h + 1) * hg]

        go_mix = [
            across(
                lambda j, h=h: w_send.at[h * hg : (h + 1) * hg],
                lambda j, h=h: w_at(h, j),
                lambda step, h=h: dp_send.at[h, step],
                lambda step, h=h: mix_recv.at[h, step],
                lambda j, h=h: needs(h)(t_own),
                lambda j, h=h: needs(h)(of(j)),
            )
            for h in range(2)
        ]
        def makes_l(t):
            return (t == k) & (yb == 1)

        def peer_w(j):
            return ((j < 2) & (lax.rem(t_own, 2) == j)) | ((j >= 2) & (t_own >= 2))

        def peer_d(j):
            return t_own == j

        def peer_l(j):
            return (t_own == j) & (lax.rem(j, 2) == 1)

        class Reduction:
            def __init__(self, makes, peer, source, refs, slot, passes):
                red, dp_sum, over, every, bulk = refs
                self.makes, self.refs, self.source = makes, refs, source
                self.to_dp = across(
                    source,
                    lambda j: red(j),
                    lambda step: dp_send.at[2 + slot, step],
                    lambda step: red_recv.at[slot],
                    lambda j: makes(of(j)),
                    lambda j: makes(t_own),
                    bulk,
                )
                self.to_span = spanning(
                    lambda j: dp_sum,
                    lambda j: over(j),
                    slot,
                    lambda j: makes(t_own),
                    lambda j: makes(t_own),
                )
                self.peer = peer
                row, column = k + 1 - 2 * yb, k + 2 - 4 * zb

                def copy(piece, at, where):
                    return remote(
                        every(piece),
                        every(piece),
                        sq_send.at[slot, at],
                        sq_recv.at[slot, at],
                        where,
                    )

                self.own_z = lambda: copy(k, 0, z_id)
                self.own_y = lambda: copy(k, 1, y_id)
                self.take_z = lambda: copy(column, 0, z_id)
                self.take_y = lambda: copy(row, 1, y_id)
                self.relays = {
                    "column": lambda: remote(
                        every(column),
                        every(column),
                        sq_send.at[slot, 2],
                        sq_recv.at[slot, 2],
                        y_id,
                    ),
                    "row": lambda: remote(
                        every(row), every(row), sq_send.at[slot, 3], sq_recv.at[slot, 2], z_id
                    ),
                }
                self.take_relay = lambda: copy(3 - k, 2, z_id)
                self.row, self.column, self.passes = row, column, passes

            def start(self):
                self.to_dp.start()

            def over_spans(self):
                red, dp_sum, over, every, _bulk = self.refs

                @pl.when(self.makes(t_own))
                def _():
                    red(d)[...] = self.source(d)[...]
                    self.to_dp.arrive()
                    dp_sum[...] = total(red, dp_count).astype(bf16)
                    self.to_span.start()
                    over(my_span)[...] = dp_sum[...]

            def pass_round(self):
                red, dp_sum, over, every, _bulk = self.refs

                @pl.when(self.makes(t_own))
                def _():
                    self.to_span.arrive()
                    every(k)[...] = total(over, spans).astype(bf16)
                    self.own_z().start()
                    self.own_y().start()

            def relay_column(self):
                @pl.when(self.peer(self.column))
                def _():
                    self.take_z().wait_recv()
                    self.relays["column"]().start()

            def relay_row(self):
                @pl.when(self.peer(self.row))
                def _():
                    self.take_y().wait_recv()
                    self.relays["row"]().start()

            def arrive(self):
                if "column" not in self.passes:
                    pl.when(self.peer(self.column))(lambda: self.take_z().wait_recv())
                if "row" not in self.passes:
                    pl.when(self.peer(self.row))(lambda: self.take_y().wait_recv())
                pl.when(self.peer(3 - k))(lambda: self.take_relay().wait_recv())

            def leave(self):
                self.to_dp.leave()
                self.to_span.leave()

                @pl.when(self.makes(t_own))
                def _():
                    self.own_z().wait_send()
                    self.own_y().wait_send()

                for way in self.passes:
                    peer = self.column if way == "column" else self.row
                    pl.when(self.peer(peer))(lambda: self.relays[way]().wait_send())

        def total(at, count):
            out = at(0)[...].astype(f32)
            for i in range(1, count):
                out = out + at(i)[...].astype(f32)
            return out

        terms_w = [
            Reduction(
                makes_w,
                peer_w,
                lambda j, i=i: term_w.at[slot_w(of(j)) * per_block + part(j), i],
                (
                    lambda j, i=i: red_w.at[i, j],
                    dp_w.at[i],
                    lambda j, i=i: span_w.at[j, i],
                    lambda j, i=i: all_w.at[j, i],
                    red_w.at[i, : dp_count - 1],
                ),
                i,
                ("column", "row") if z == 1 else (),
            )
            for i in range(hg)
        ]
        terms_d = Reduction(
            makes_n,
            peer_d,
            lambda j: term_d.at[part(j)],
            (
                lambda j: red_d.at[j],
                dp_d,
                lambda j: span_d.at[j],
                lambda j: all_d.at[j],
                red_d.at[: dp_count - 1],
            ),
            hg,
            ("column", "row") if z == 1 else (),
        )
        terms_l = Reduction(
            makes_l,
            peer_l,
            lambda j: term_l.at[part(j)],
            (
                lambda j: red_l.at[j],
                dp_l,
                lambda j: span_l.at[j],
                lambda j: all_l.at[j],
                red_l.at[: dp_count - 1],
            ),
            hg + 1,
            ("column",),
        )

        def vec(at):
            return lambda step: vec_sems.at[at]

        late_go = (
            across(
                lambda j: late_s.at[0],
                lambda j: late_a.at[j],
                vec(0),
                vec(1),
                bulk=late_a.at[: dp_count - 1],
            ),
            Exchange(
                lambda j: late_s.at[1],
                lambda j: late_b.at[j],
                me,
                spans * QUAD,
                sp_id,
                vec(2),
                vec(3),
                bulk=late_b.at[: spans * QUAD - 1],
            ),
        )
        early_go = (
            across(
                lambda j: early_s.at[0],
                lambda j: early_a.at[j],
                vec(4),
                vec(5),
                bulk=early_a.at[: dp_count - 1],
            ),
            Exchange(
                lambda j: early_s.at[1],
                lambda j: early_c.at[j],
                me // 2,
                spans * QUAD // 2,
                lambda j: {"sp": 2 * j + lax.rem(me, 2)},
                vec(6),
                vec(7),
                bulk=early_c.at[: spans * QUAD // 2 - 1],
            ),
            Exchange(
                lambda j: early_s.at[2],
                lambda j: early_b.at[j],
                lax.rem(me, 2),
                2,
                lambda j: {"sp": me - lax.rem(me, 2) + j},
                vec(8),
                vec(9),
            ),
        )

        def make_normed():
            for fetch in (fetches[4], fetches[5], fetches[2]):
                fetch.wait()

            @pl.loop(0, tok // CHUNK, unroll=4)
            def _(r):
                at = piece(r)
                raw = values[at, :].astype(f32)
                centred = raw - jnp.mean(raw, axis=-1, keepdims=True)
                inv_std = lax.rsqrt(jnp.mean(centred * centred, axis=-1, keepdims=True) + EPS)
                one = centred * inv_std
                unit[at, :] = one
                inv[at, :] = jnp.broadcast_to(inv_std, (CHUNK, 128))
                normed = (one * gain[...] + shift[...]).astype(bf16)
                for g in range(groups):
                    nbuf[g, n_own[g], at, :] = normed[:, lanes_of(g)]

        def make_cotangent():
            fetches[0].wait()
            fetches[1].wait()

            @pl.loop(0, tok // CHUNK)
            def _(r):
                at = piece(r)
                prod = (upstream[at, :].astype(f32) * gated[at, :].astype(f32)).astype(bf16)
                for g in range(groups):
                    gbuf[g, g_own[g], at, :] = prod[:, lanes_of(g)]

        def meet():
            pl.semaphore_wait(barrier, spans * QUAD + dp_count - 2)

        def narrow_n():
            @pl.when(yb == 0)
            def _():
                for g in narrow:
                    narrow_y(nbuf, 0, g).start()

        def narrow_g():
            @pl.when(yb == 1)
            def _():
                for g in narrow:
                    narrow_y(gbuf, 1, g).start()

        (make_normed if z == 0 else make_cotangent)()
        meet()
        for g, h in zip(wide, narrow):
            y_send[g].start()
            z_send[h].start()
        (narrow_n if z == 0 else narrow_g)()
        (make_cotangent if z == 0 else make_normed)()
        (narrow_g if z == 0 else narrow_n)()

        @pl.when(yb == 0)
        def _():
            for g in narrow:
                nbuf[g, 1] = jnp.zeros((tok, width), bf16)

        @pl.when(yb == 1)
        def _():
            for g in narrow:
                gbuf[g, 0] = jnp.zeros((tok, width), bf16)

        fetches[3].wait()

        @pl.loop(0, rows // CHUNK)
        def _(r):
            at = piece(r)
            for c in range(2):
                for h in range(2):
                    if z == 0:
                        col = c
                    elif h == 0:
                        col = 2 + c
                    else:
                        col = yb + 2 * c
                    start = col * tok
                    if not isinstance(start, int):
                        start = pl.multiple_of(start, tok)
                    block = mix_w[at, :, pl.ds(start, tok)].astype(f32)
                    keep = allowed(d * rows + r * CHUNK, col * tok, CHUNK, tok)
                    for g in range(h * hg, (h + 1) * hg):
                        w_send[g, at, c * tok : (c + 1) * tok] = jnp.where(
                            keep, block[:, g, :], 0.0
                        ).astype(bf16)

        for h in (z, 1 - z):
            go_mix[h].start()

            @pl.when(needs(h)(t_own))
            def _():
                w_at(h, d)[...] = w_send[h * hg : (h + 1) * hg]

        for i, g in enumerate(narrow):
            block = nt(gbuf[g, g_own[g]], nbuf[g, n_own[g]])
            kept = jnp.where(allowed(0, 0, tok, tok), block, 0.0).astype(bf16)
            for p in range(per_block):
                term_d[p, i] = kept[p * rows : (p + 1) * rows]
        terms_d.start()

        fetches[6].wait()
        own_bias = mix_bias[:, 0:tok]
        for b in range(1, QUAD):
            own_bias = jnp.where(k == b, mix_bias[:, b * tok : (b + 1) * tok], own_bias)
        for g in range(groups):
            bias_t[g] = jnp.transpose(jnp.broadcast_to(own_bias[g : g + 1], (128, tok)))
        acc_gain[...] = jnp.zeros_like(acc_gain)
        acc_shift[...] = jnp.zeros_like(acc_shift)
        sum_a[...] = jnp.zeros_like(sum_a)
        sum_b[...] = jnp.zeros_like(sum_b)
        grad_mix[...] = jnp.zeros_like(grad_mix)
        lines = hg * width // 128
        per_span = span // 128
        for g in range(groups):
            bias_sum = nt(jnp.ones((8, width), bf16), gbuf[g, g_own[g]])[0:1]
            for b in range(QUAD):
                shown = jnp.where(k == b, bias_sum, 0.0)
                for c in range(tok // 128):
                    at = 2 * lines + g * per_span + b * (tok // 128) + c
                    early_s[0, at : at + 1, :] = shown[:, c * 128 : (c + 1) * 128]

        def give_u(g, mixed):
            for c in range(width // 128):
                lanes = slice(c * 128, (c + 1) * 128)
                at = slice(g * width + c * 128, g * width + (c + 1) * 128)
                whole = (mixed[:, lanes] + bias_t[g]).astype(bf16).astype(f32)
                grad_u[:, at] = (upstream[:, at].astype(f32) * whole).astype(bf16)

        def give_back(g, total):
            back[g] = total.astype(bf16)

            @pl.loop(0, tok // CHUNK)
            def _(r):
                at = piece(r)
                grad_normed = back[g, at, :].astype(f32)
                one = unit[at, lanes_of(g)]
                prod = grad_normed * one
                acc_gain[:, lanes_of(g)] += prod[0:8] + prod[8:16]
                acc_shift[:, lanes_of(g)] += grad_normed[0:8] + grad_normed[8:16]
                scaled = grad_normed * gain[:, lanes_of(g)]
                prod = scaled * one
                a, b = scaled[:, 0:128], prod[:, 0:128]
                for c in range(1, width // 128):
                    a = a + scaled[:, c * 128 : (c + 1) * 128]
                    b = b + prod[:, c * 128 : (c + 1) * 128]
                sum_a[at, :] += a
                sum_b[at, :] += b

        def give_v():
            @pl.loop(0, tok // CHUNK)
            def _(r):
                at = piece(r)
                mean_a = jnp.sum(sum_a[at, :], axis=-1, keepdims=True) / half
                mean_b = jnp.sum(sum_b[at, :], axis=-1, keepdims=True) / half
                inv_std = inv[at, :][:, 0:1]
                for g in range(groups):
                    scaled = back[g, at, :].astype(f32) * gain[:, lanes_of(g)]
                    grad_v[at, lanes_of(g)] = (
                        inv_std * (scaled - mean_a - unit[at, lanes_of(g)] * mean_b)
                    ).astype(bf16)

        def own_cols(g, block):
            at = pl.ds(pl.multiple_of(block * tok, tok), tok)
            return w_block[:, g, :, at].reshape(2 * tok, tok)

        def own_rows(g, block):
            return w_block[pl.ds(block * per_block, per_block), g].reshape(tok, 2 * tok)

        def pair(buf, g):
            return buf[g].reshape(2 * tok, width)

        def keep_of(row, col):
            return allowed(row * tok, col * tok, tok, tok)

        def gather_sums(h, out):
            first = h * hg * width
            for ref, line in ((acc_gain, 0), (acc_shift, lines)):
                whole = jnp.sum(ref[:, first : first + hg * width], axis=0, keepdims=True)
                for i in range(lines):
                    out[0, line + i : line + i + 1, :] = whole[:, i * 128 : (i + 1) * 128]

        def send_early():
            gather_sums(1, early_s)
            early_go[0].start()
            early_a[d] = early_s[0]

        def spread_early():
            early_go[0].arrive()
            early_s[1] = total(lambda j: early_a.at[j], dp_count)
            early_go[1].start()
            early_c[me // 2] = early_s[1]

        def respread_early():
            early_go[1].arrive()
            early_s[2] = total(lambda j: early_c.at[j], spans * QUAD // 2)
            early_go[2].start()
            early_b[lax.rem(me, 2)] = early_s[2]

        def send_late():
            gather_sums(0, late_s)
            late_go[0].start()
            late_a[d] = late_s[0]

        def spread_late():
            late_go[0].arrive()
            late_s[1] = total(lambda j: late_a.at[j], dp_count)
            late_go[1].start()
            late_b[me] = late_s[1]

        def put_sums(h, whole):
            for i in range(lines):
                to = slice((h * lines + i) * 128, (h * lines + i + 1) * 128)
                grad_gain[:, to] = whole[i : i + 1]
                grad_shift[:, to] = whole[lines + i : lines + i + 1]

        def take_early():
            early_go[2].arrive()
            whole = total(lambda j: early_b.at[j], 2)
            put_sums(1, whole)
            for g in range(groups):
                for c in range(per_span):
                    at = 2 * lines + g * per_span + c
                    grad_bias[g : g + 1, c * 128 : (c + 1) * 128] = whole[at : at + 1]

        def take_late():
            late_go[1].arrive()
            put_sums(0, total(lambda j: late_b.at[j], spans * QUAD))

        go_mix[z].arrive()
        for i, g in enumerate(wide):
            y_take[g].wait_recv()
            if z == 0:
                both = nn(w_block[:, g].reshape(2 * tok, 2 * tok), pair(nbuf, g))
                stage_z[i] = both[tok:].astype(bf16)
                pz[i].start()
                give_u(g, both[:tok])
            else:
                both = tn(w_block[:, g].reshape(2 * tok, 2 * tok), pair(gbuf, g))
                stage_z[i] = both[:tok].astype(bf16)
                pz[i].start()
                give_back(g, both[tok:])
            z_take[g].wait_recv()
            if z == 0:
                stage_y[i] = tn(own_cols(g, 1 - yb), pair(gbuf, g)).astype(bf16)
            else:
                stage_y[i] = nn(own_rows(g, 1 - yb), pair(nbuf, g)).astype(bf16)
            if z == 0 or i < hg - 1:
                py[i].start()
            block = nt(pair(gbuf, g), pair(nbuf, g))
            for a in range(2):
                for b in range(2):
                    if z == 0:
                        keep = keep_of(yb + 2 * a, b)
                    else:
                        keep = keep_of(2 + a, yb + 2 * b)
                    at, of_s = slice(a * tok, (a + 1) * tok), slice(b * tok, (b + 1) * tok)
                    kept = jnp.where(keep, block[at, of_s], 0.0).astype(bf16)
                    for p in range(per_block):
                        term_w[a * per_block + p, i, :, of_s] = kept[p * rows : (p + 1) * rows]
            terms_w[i].start()
            if z == 0:
                own_part[i] = tn(own_cols(g, yb), pair(gbuf, g))
            else:
                own_part[i] = nn(own_rows(g, yb), pair(nbuf, g))

        go_mix[1 - z].arrive()
        terms_d.over_spans()
        for i, g in enumerate(narrow):
            terms_w[i].over_spans()

            @pl.when(yb == 1)
            def _():
                narrow_y(nbuf, 0, g).wait_recv()
                block = nt(gbuf[g, g_own[g]], nbuf[g, 0]).astype(bf16)
                for p in range(per_block):
                    term_l[p, i] = block[p * rows : (p + 1) * rows]

            @pl.when(yb == 0)
            def _():
                narrow_y(gbuf, 1, g).wait_recv()

            if i == hg - 1:
                terms_l.start()
            if z == 0:
                give_u(g, nn(own_rows(g, yb), pair(nbuf, g)))
            pz[i].wait_recv()
            if z == 0:
                give_back(g, recv_z[i].astype(f32) + tn(own_cols(g, yb), pair(gbuf, g)))
            else:
                give_back(g, tn(own_cols(g, yb), pair(gbuf, g)))
                give_u(g, recv_z[i].astype(f32) + nn(own_rows(g, yb), pair(nbuf, g)))

        send_early()
        if z == 1:
            send_late()
        terms_d.pass_round()
        for term in terms_w:
            term.pass_round()
        if z == 1:
            give_v()
        if z == 1:
            for term in (terms_d, *terms_w):
                term.relay_column()
            py[hg - 1].start()
        terms_l.over_spans()
        spread_early()
        if z == 1:
            spread_late()

        for i, g in enumerate(wide):
            if z == 1 and i == hg - 1:
                for term in (terms_d, *terms_w):
                    term.relay_row()
                respread_early()
                terms_l.pass_round()
            py[i].wait_recv()
            whole = own_part[i] + recv_y[i].astype(f32)
            if z == 0:
                give_back(g, whole)
            else:
                give_u(g, whole)
        if z == 0:
            send_late()
            terms_l.pass_round()
            respread_early()
            terms_l.relay_column()
            spread_late()
            give_v()
        else:
            terms_l.relay_column()

        def put(g, first, block):
            grad_mix[:, g, first * tok : first * tok + block.shape[1]] = block.astype(f32)

        for g in wide:
            y_send[g].wait_send()
        for g in narrow:
            z_send[g].wait_send()

            @pl.when(yb == 0)
            def _():
                narrow_y(nbuf, 0, g).wait_send()

            @pl.when(yb == 1)
            def _():
                narrow_y(gbuf, 1, g).wait_send()

        for i in range(hg):
            py[i].wait_send()
            pz[i].wait_send()
        for go in (*go_mix, late_go[0], early_go[0]):
            go.leave()

        terms_d.arrive()
        for t in range(QUAD):

            @pl.when(t_own == t)
            def _():
                for i in range(hg):
                    put(i if t >= 2 else hg + i, t, all_d[t, i])

        terms_d.leave()
        for i, term in enumerate(terms_w):
            term.arrive()
            put(i, 0, all_w[lax.rem(t_own, 2), i])

            @pl.when(t_own >= 2)
            def _():
                for b in range(2):
                    put(hg + i, b, all_w[2 + b, i][:, :tok])

            for t in range(2, QUAD):

                @pl.when(t_own == t)
                def _():
                    for b in range(t - 1):
                        put(hg + i, b + 2, all_w[2 + b, i][:, tok:])

            term.leave()
        terms_l.arrive()
        for t in range(1, QUAD, 2):

            @pl.when(t_own == t)
            def _():
                for i in range(hg):
                    put(i if t >= 2 else hg + i, t - 1, all_l[t, i])

        terms_l.leave()
        take_early()
        for go in early_go[1:]:
            go.leave()
        take_late()
        late_go[1].leave()

    for z in range(2):
        pl.when(zb == z)(functools.partial(run, z))


def finish(*refs):
    count = len(refs) // 2
    sems = refs[-1]
    copies = [
        pltpu.make_async_copy(src, dst, sems.at[i])
        for i, (src, dst) in enumerate(zip(refs[:count], refs[count : 2 * count]))
    ]
    for copy in copies:
        copy.start()
    for copy in copies:
        copy.wait()


def per_device(gated, values_in, upstream, gain, shift, mix_w, mix_bias):
    dp_count = lax.axis_size("dp")
    sp_count = lax.axis_size("sp")
    tok, half = gated.shape[1:]
    rows, groups, span = mix_w.shape
    width = half // groups
    assert span == QUAD * tok and groups % 2 == 0 and tok % rows == 0
    spans = sp_count // QUAD
    hg = groups // 2
    f32, bf16 = jnp.float32, jnp.bfloat16
    hbm = pl.BlockSpec(memory_space=pltpu.HBM)
    vmem = pl.BlockSpec(memory_space=pltpu.VMEM)
    dma = pltpu.SemaphoreType.DMA
    term, slim = (hg, rows, 2 * tok), (hg, rows, tok)
    late_rows = half // 128
    early_rows = late_rows + groups * span // 128
    assert half % 256 == 0 and tok % 128 == 0
    scratch = (
        [pltpu.VMEM((tok, half), bf16)] * 3
        + [
            pltpu.VMEM((rows, groups, span), bf16),
            pltpu.VMEM((1, half), f32),
            pltpu.VMEM((1, half), f32),
            pltpu.VMEM((groups, span), f32),
            pltpu.VMEM((tok, half), f32),
            pltpu.VMEM((tok, 128), f32),
            pltpu.VMEM((groups, 2, tok, width), bf16),
            pltpu.VMEM((groups, 2, tok, width), bf16),
            pltpu.VMEM((groups, rows, 2 * tok), bf16),
            pltpu.VMEM((2 * (tok // rows), groups, rows, 2 * tok), bf16),
        ]
        + [pltpu.VMEM((hg, tok, width), bf16)] * 4
        + [
            pltpu.VMEM((hg, tok, width), f32),
            pltpu.VMEM((groups, tok, width), bf16),
            pltpu.VMEM((tok, 128), f32),
            pltpu.VMEM((tok, 128), f32),
            pltpu.VMEM((8, half), f32),
            pltpu.VMEM((8, half), f32),
            pltpu.VMEM((2 * (tok // rows),) + term, bf16),
            pltpu.VMEM((tok // rows,) + slim, bf16),
            pltpu.VMEM((tok // rows,) + slim, bf16),
        ]
        + [pltpu.VMEM((hg, dp_count, rows, 2 * tok), bf16)]
        + [pltpu.VMEM((dp_count,) + shape, bf16) for shape in (slim, slim)]
        + [pltpu.VMEM(shape, bf16) for shape in (term, slim, slim)]
        + [pltpu.VMEM((spans,) + shape, bf16) for shape in (term, slim, slim)]
        + [pltpu.VMEM((QUAD,) + shape, bf16) for shape in (term, slim, slim)]
        + [
            pltpu.VMEM((2, late_rows, 128), f32),
            pltpu.VMEM((dp_count, late_rows, 128), f32),
            pltpu.VMEM((sp_count, late_rows, 128), f32),
            pltpu.VMEM((3, early_rows, 128), f32),
            pltpu.VMEM((dp_count, early_rows, 128), f32),
            pltpu.VMEM((2, early_rows, 128), f32),
            pltpu.VMEM((sp_count // 2, early_rows, 128), f32),
            pltpu.VMEM((groups, tok, 128), f32),
        ]
        + [dma((2, groups)), dma((4, hg)), dma((2, hg))]
        + [dma((4 + hg, dp_count - 1)), dma((2, dp_count - 1)), dma((2 + hg,)), dma((10,))]
        + [dma((2 + hg, spans - 1))] * 2
        + [dma((2 + hg, 4)), dma((2 + hg, 3))]
        + [dma((7,))]
    )
    shapes = (
        jax.ShapeDtypeStruct((tok, half), bf16),
        jax.ShapeDtypeStruct((tok, half), bf16),
        jax.ShapeDtypeStruct((rows, groups, span), f32),
        jax.ShapeDtypeStruct((1, half), f32),
        jax.ShapeDtypeStruct((1, half), f32),
        jax.ShapeDtypeStruct((groups, span), f32),
    )
    out = pl.pallas_call(
        functools.partial(kernel, (tok, width, groups, span, dp_count, spans)),
        out_shape=shapes,
        in_specs=[hbm] * 7,
        out_specs=[vmem] * 6,
        scratch_shapes=scratch,
        compiler_params=pltpu.CompilerParams(
            collective_id=0, has_side_effects=True, vmem_limit_bytes=36 * 1024 * 1024
        ),
    )(
        *(
            pltpu.with_memory_space_constraint(x, pltpu.HBM)
            for x in (
                gated[0],
                values_in[0],
                upstream[0],
                gain[None],
                shift[None],
                mix_w,
                mix_bias,
            )
        )
    )
    u, v, mix, gain_g, shift_g, bias = pl.pallas_call(
        finish,
        out_shape=shapes,
        in_specs=[vmem] * 6,
        out_specs=[hbm] * 6,
        scratch_shapes=[dma((6,))],
        compiler_params=pltpu.CompilerParams(vmem_limit_bytes=36 * 1024 * 1024),
    )(*out)
    return (u[None], v[None], mix, bias, gain_g[0], shift_g[0])


def solution(mesh):
    placed = (
        P("dp", "sp", None),
        P("dp", "sp", None),
        P("dp", "sp", None),
        P(),
        P(),
        P("dp", None, None),
        P(),
    )
    return jax.shard_map(
        per_device,
        mesh=mesh,
        in_specs=placed,
        out_specs=(P("dp", "sp", None), P("dp", "sp", None), P("dp", None, None), P(), P(), P()),
        check_vma=False,
    )
```

```python
import functools

import jax
import jax.numpy as jnp
from jax import lax
from jax.experimental import pallas as pl
from jax.experimental.pallas import tpu as pltpu
from jax.sharding import PartitionSpec as P

SEG = 64

EPS = 1e-05

CHUNK = 16

QUAD = 4


def nt(a, b):
    return lax.dot_general(a, b, (((1,), (1,)), ((), ())), preferred_element_type=jnp.float32)


def tn(a, b):
    return lax.dot_general(a, b, (((0,), (0,)), ((), ())), preferred_element_type=jnp.float32)


def nn(a, b):
    return jnp.dot(a, b, preferred_element_type=jnp.float32)


def kernel(
    dims,
    gated_in,
    values_in,
    upstream_in,
    gain_in,
    shift_in,
    mix_in,
    bias_in,
    grad_u,
    grad_v,
    grad_mix,
    grad_gain,
    grad_shift,
    grad_bias,
    gated,
    values,
    upstream,
    mix_w,
    gain,
    shift,
    mix_bias,
    unit,
    inv,
    nbuf,
    gbuf,
    w_send,
    w_block,
    stage_y,
    stage_z,
    recv_y,
    recv_z,
    own_part,
    back,
    sum_a,
    sum_b,
    acc_gain,
    acc_shift,
    term_w,
    term_d,
    term_l,
    red_w,
    red_d,
    red_l,
    dp_w,
    dp_d,
    dp_l,
    span_w,
    span_d,
    span_l,
    all_w,
    all_d,
    all_l,
    late_s,
    late_a,
    late_b,
    early_s,
    early_a,
    early_b,
    early_c,
    bias_t,
    raw_sems,
    part_sems,
    z_sems,
    dp_send,
    mix_recv,
    red_recv,
    vec_sems,
    sn_send,
    sn_recv,
    sq_send,
    sq_recv,
    in_sem,
):
    tok, width, groups, span, dp_count, spans = dims
    half = groups * width
    rows = span // dp_count
    per_block = tok // rows
    hg = groups // 2
    me = lax.axis_index("sp")
    my_span, k = me // QUAD, lax.rem(me, QUAD)
    zb, yb = k // 2, lax.rem(k, 2)
    d = lax.axis_index("dp")
    t_own = d // per_block
    f32, bf16 = jnp.float32, jnp.bfloat16

    def sq_id(j):
        return {"sp": my_span * QUAD + j}

    def dp_id(j):
        return {"dp": j}

    def sn_id(j):
        return {"sp": j * QUAD + k}

    def sp_id(j):
        return {"sp": j}

    y_id = sq_id(k + 1 - 2 * yb)
    z_id = sq_id(k + 2 - 4 * zb)

    def remote(src, dst, send, recv, where):
        return pltpu.make_async_remote_copy(
            src_ref=src,
            dst_ref=dst,
            send_sem=send,
            recv_sem=recv,
            device_id=where,
            device_id_type=pl.DeviceIdType.MESH,
        )

    class Exchange:
        def __init__(
            self, src, dst, own, count, where, send, recv, gives=None, takes=None, bulk=None
        ):
            self.src, self.dst, self.own, self.count = src, dst, own, count
            self.where, self.send, self.recv = where, send, recv
            self.gives, self.takes, self.bulk = gives, takes, bulk

        def copy(self, step, to):
            peer = lax.rem(self.own + step, self.count)
            landing = self.own if to else peer
            by = step if to else self.count - step
            return remote(
                self.src(peer) if to else self.dst(landing),
                self.dst(landing),
                self.send(step - 1),
                self.recv(by - 1),
                self.where(peer),
            )

        def each(self, cond, act):
            for step in range(1, self.count):
                if cond is None:
                    act(step)
                else:
                    pl.when(cond(lax.rem(self.own + step, self.count)))(lambda: act(step))

        def all_of_it(self):
            where = self.where(lax.rem(self.own + 1, self.count))
            return remote(self.bulk, self.bulk, self.send(0), self.recv(0), where)

        def start(self):
            self.each(self.gives, lambda step: self.copy(step, True).start())

        def arrive(self):
            if self.bulk is None:
                self.each(self.takes, lambda step: self.copy(step, False).wait_recv())
            elif self.takes is None:
                self.all_of_it().wait_recv()
            else:
                pl.when(self.takes(self.own))(lambda: self.all_of_it().wait_recv())

        def leave(self):
            if self.bulk is None or self.gives is not None:
                self.each(self.gives, lambda step: self.copy(step, True).wait_send())
            else:
                self.all_of_it().wait_send()

    def across(src, dst, send, recv, gives=None, takes=None, bulk=None):
        return Exchange(src, dst, d, dp_count, dp_id, send, recv, gives, takes, bulk)

    def spanning(src, dst, slot, gives=None, takes=None):
        return Exchange(
            src,
            dst,
            my_span,
            spans,
            sn_id,
            lambda step: sn_send.at[slot, step],
            lambda step: sn_recv.at[slot, step],
            gives,
            takes,
        )

    fetches = [
        pltpu.make_async_copy(src, dst, in_sem.at[i])
        for i, (src, dst) in enumerate(
            (
                (gated_in, gated),
                (upstream_in, upstream),
                (values_in, values),
                (mix_in, mix_w),
                (gain_in, gain),
                (shift_in, shift),
                (bias_in, mix_bias),
            )
        )
    ]
    for z, order in ((0, (4, 5, 2, 0, 1, 3, 6)), (1, (0, 1, 2, 4, 5, 3, 6))):

        @pl.when(zb == z)
        def _():
            for i in order:
                fetches[i].start()

    barrier = pltpu.get_barrier_semaphore()
    for own, count, where in ((me, spans * QUAD, sp_id), (d, dp_count, dp_id)):
        for step in range(1, count):
            pl.semaphore_signal(
                barrier,
                inc=1,
                device_id=where(lax.rem(own + step, count)),
                device_id_type=pl.DeviceIdType.MESH,
            )

    def piece(r):
        return pl.ds(pl.multiple_of(r * CHUNK, CHUNK), CHUNK)

    def lanes_of(g):
        return slice(g * width, (g + 1) * width)

    def allowed(first_t, first_s, n_t, n_s):
        t = first_t + lax.broadcasted_iota(jnp.int32, (n_t, n_s), 0)
        s = first_s + lax.broadcasted_iota(jnp.int32, (n_t, n_s), 1)
        return lax.div(t, SEG) >= lax.div(s, SEG)

    def run(z):
        first = range(hg)
        second = range(hg, groups)
        wide = first if z == 0 else second
        narrow = second if z == 0 else first
        n_own = {g: yb if (z == 0 or g in first) else 1 for g in range(groups)}
        g_own = {g: yb if (z == 1 or g in second) else 0 for g in range(groups)}

        def makes_w(t):
            return (lax.rem(t, 2) == yb) if z == 0 else (t >= 2)

        def slot_w(t):
            return lax.div(t, 2) if z == 0 else t - 2

        def makes_n(t):
            return t == k

        def of(j):
            return j // per_block

        def part(j):
            return lax.rem(j, per_block)

        x_buf = nbuf if z == 0 else gbuf
        o_buf = gbuf if z == 0 else nbuf
        raw_y = {}
        for g in wide:
            raw_y[g] = x_buf
        y_send = {
            g: remote(
                x_buf.at[g, yb], x_buf.at[g, yb], raw_sems.at[0, g], raw_sems.at[1, g], y_id
            )
            for g in wide
        }
        y_take = {
            g: remote(
                x_buf.at[g, 1 - yb],
                x_buf.at[g, 1 - yb],
                raw_sems.at[0, g],
                raw_sems.at[1, g],
                y_id,
            )
            for g in wide
        }

        def narrow_y(buf, slot, g):
            return remote(
                buf.at[g, slot], buf.at[g, slot], raw_sems.at[0, g], raw_sems.at[1, g], y_id
            )

        z_buf = nbuf if z == 0 else gbuf
        z_own = n_own if z == 0 else g_own
        z_slot = 0 if z == 0 else 1
        z_send = {
            g: remote(
                z_buf.at[g, z_own[g]],
                z_buf.at[g, z_slot],
                z_sems.at[0, i],
                z_sems.at[1, i],
                z_id,
            )
            for i, g in enumerate(narrow)
        }
        z_take = {
            g: remote(
                o_buf.at[g, 1 - z_slot],
                o_buf.at[g, 1 - z_slot],
                z_sems.at[0, i],
                z_sems.at[1, i],
                z_id,
            )
            for i, g in enumerate(wide)
        }
        py = [
            remote(stage_y.at[i], recv_y.at[i], part_sems.at[0, i], part_sems.at[1, i], y_id)
            for i in range(hg)
        ]
        pz = [
            remote(stage_z.at[i], recv_z.at[i], part_sems.at[2, i], part_sems.at[3, i], z_id)
            for i in range(hg)
        ]

        def needs(h):
            return makes_w if h == z else ((lambda t: t < 2) if z == 0 else (lambda t: t >= 2))

        def slot_of(h, t):
            return slot_w(t) if h == z else (t if z == 0 else t - 2)

        def w_at(h, j):
            return w_block.at[slot_of(h, of(j)) * per_block + part(j), h * hg : (h + 1) * hg]

        go_mix = [
            across(
                lambda j, h=h: w_send.at[h * hg : (h + 1) * hg],
                lambda j, h=h: w_at(h, j),
                lambda step, h=h: dp_send.at[h, step],
                lambda step, h=h: mix_recv.at[h, step],
                lambda j, h=h: needs(h)(t_own),
                lambda j, h=h: needs(h)(of(j)),
            )
            for h in range(2)
        ]
        def makes_l(t):
            return (t == k) & (yb == 1)

        def peer_w(j):
            return ((j < 2) & (lax.rem(t_own, 2) == j)) | ((j >= 2) & (t_own >= 2))

        def peer_d(j):
            return t_own == j

        def peer_l(j):
            return (t_own == j) & (lax.rem(j, 2) == 1)

        class Reduction:
            def __init__(self, makes, peer, source, refs, slot, passes):
                red, dp_sum, over, every, bulk = refs
                self.makes, self.refs, self.source = makes, refs, source
                self.to_dp = across(
                    source,
                    lambda j: red(j),
                    lambda step: dp_send.at[2 + slot, step],
                    lambda step: red_recv.at[slot],
                    lambda j: makes(of(j)),
                    lambda j: makes(t_own),
                    bulk,
                )
                self.to_span = spanning(
                    lambda j: dp_sum,
                    lambda j: over(j),
                    slot,
                    lambda j: makes(t_own),
                    lambda j: makes(t_own),
                )
                self.peer = peer
                row, column = k + 1 - 2 * yb, k + 2 - 4 * zb

                def copy(piece, at, where):
                    return remote(
                        every(piece),
                        every(piece),
                        sq_send.at[slot, at],
                        sq_recv.at[slot, at],
                        where,
                    )

                self.own_z = lambda: copy(k, 0, z_id)
                self.own_y = lambda: copy(k, 1, y_id)
                self.take_z = lambda: copy(column, 0, z_id)
                self.take_y = lambda: copy(row, 1, y_id)
                self.relays = {
                    "column": lambda: remote(
                        every(column),
                        every(column),
                        sq_send.at[slot, 2],
                        sq_recv.at[slot, 2],
                        y_id,
                    ),
                    "row": lambda: remote(
                        every(row), every(row), sq_send.at[slot, 3], sq_recv.at[slot, 2], z_id
                    ),
                }
                self.take_relay = lambda: copy(3 - k, 2, z_id)
                self.row, self.column, self.passes = row, column, passes

            def start(self):
                self.to_dp.start()

            def over_spans(self):
                red, dp_sum, over, every, _bulk = self.refs

                @pl.when(self.makes(t_own))
                def _():
                    red(d)[...] = self.source(d)[...]
                    self.to_dp.arrive()
                    dp_sum[...] = total(red, dp_count).astype(bf16)
                    self.to_span.start()
                    over(my_span)[...] = dp_sum[...]

            def pass_round(self, along_y=True):
                red, dp_sum, over, every, _bulk = self.refs

                @pl.when(self.makes(t_own))
                def _():
                    self.to_span.arrive()
                    every(k)[...] = total(over, spans).astype(bf16)
                    self.own_z().start()
                    if along_y:
                        self.own_y().start()

            def pass_along_y(self):
                pl.when(self.makes(t_own))(lambda: self.own_y().start())

            def relay_column(self):
                @pl.when(self.peer(self.column))
                def _():
                    self.take_z().wait_recv()
                    self.relays["column"]().start()

            def relay_row(self):
                @pl.when(self.peer(self.row))
                def _():
                    self.take_y().wait_recv()
                    self.relays["row"]().start()

            def arrive(self):
                if "column" not in self.passes:
                    pl.when(self.peer(self.column))(lambda: self.take_z().wait_recv())
                if "row" not in self.passes:
                    pl.when(self.peer(self.row))(lambda: self.take_y().wait_recv())
                pl.when(self.peer(3 - k))(lambda: self.take_relay().wait_recv())

            def leave(self):
                self.to_dp.leave()
                self.to_span.leave()

                @pl.when(self.makes(t_own))
                def _():
                    self.own_z().wait_send()
                    self.own_y().wait_send()

                for way in self.passes:
                    peer = self.column if way == "column" else self.row
                    pl.when(self.peer(peer))(lambda: self.relays[way]().wait_send())

        def total(at, count):
            out = at(0)[...].astype(f32)
            for i in range(1, count):
                out = out + at(i)[...].astype(f32)
            return out

        terms_w = [
            Reduction(
                makes_w,
                peer_w,
                lambda j, i=i: term_w.at[slot_w(of(j)) * per_block + part(j), i],
                (
                    lambda j, i=i: red_w.at[i, j],
                    dp_w.at[i],
                    lambda j, i=i: span_w.at[j, i],
                    lambda j, i=i: all_w.at[j, i],
                    red_w.at[i, : dp_count - 1],
                ),
                i,
                ("column", "row") if z == 1 else (),
            )
            for i in range(hg)
        ]
        terms_d = Reduction(
            makes_n,
            peer_d,
            lambda j: term_d.at[part(j)],
            (
                lambda j: red_d.at[j],
                dp_d,
                lambda j: span_d.at[j],
                lambda j: all_d.at[j],
                red_d.at[: dp_count - 1],
            ),
            hg,
            ("column", "row") if z == 1 else (),
        )
        terms_l = Reduction(
            makes_l,
            peer_l,
            lambda j: term_l.at[part(j)],
            (
                lambda j: red_l.at[j],
                dp_l,
                lambda j: span_l.at[j],
                lambda j: all_l.at[j],
                red_l.at[: dp_count - 1],
            ),
            hg + 1,
            ("column",),
        )

        def vec(at):
            return lambda step: vec_sems.at[at]

        late_go = (
            across(
                lambda j: late_s.at[0],
                lambda j: late_a.at[j],
                vec(0),
                vec(1),
                bulk=late_a.at[: dp_count - 1],
            ),
            Exchange(
                lambda j: late_s.at[1],
                lambda j: late_b.at[j],
                me,
                spans * QUAD,
                sp_id,
                vec(2),
                vec(3),
                bulk=late_b.at[: spans * QUAD - 1],
            ),
        )
        early_go = (
            across(
                lambda j: early_s.at[0],
                lambda j: early_a.at[j],
                vec(4),
                vec(5),
                bulk=early_a.at[: dp_count - 1],
            ),
            Exchange(
                lambda j: early_s.at[1],
                lambda j: early_c.at[j],
                me // 2,
                spans * QUAD // 2,
                lambda j: {"sp": 2 * j + lax.rem(me, 2)},
                vec(6),
                vec(7),
                bulk=early_c.at[: spans * QUAD // 2 - 1],
            ),
            Exchange(
                lambda j: early_s.at[2],
                lambda j: early_b.at[j],
                lax.rem(me, 2),
                2,
                lambda j: {"sp": me - lax.rem(me, 2) + j},
                vec(8),
                vec(9),
            ),
        )

        def make_normed():
            for fetch in (fetches[4], fetches[5], fetches[2]):
                fetch.wait()

            @pl.loop(0, tok // CHUNK, unroll=4)
            def _(r):
                at = piece(r)
                raw = values[at, :].astype(f32)
                centred = raw - jnp.mean(raw, axis=-1, keepdims=True)
                inv_std = lax.rsqrt(jnp.mean(centred * centred, axis=-1, keepdims=True) + EPS)
                one = centred * inv_std
                unit[at, :] = one
                inv[at, :] = jnp.broadcast_to(inv_std, (CHUNK, 128))
                normed = (one * gain[...] + shift[...]).astype(bf16)
                for g in range(groups):
                    nbuf[g, n_own[g], at, :] = normed[:, lanes_of(g)]

        def make_cotangent():
            fetches[0].wait()
            fetches[1].wait()

            @pl.loop(0, tok // CHUNK)
            def _(r):
                at = piece(r)
                prod = (upstream[at, :].astype(f32) * gated[at, :].astype(f32)).astype(bf16)
                for g in range(groups):
                    gbuf[g, g_own[g], at, :] = prod[:, lanes_of(g)]

        def meet():
            pl.semaphore_wait(barrier, spans * QUAD + dp_count - 2)

        def narrow_n():
            @pl.when(yb == 0)
            def _():
                for g in narrow:
                    narrow_y(nbuf, 0, g).start()

        def narrow_g():
            @pl.when(yb == 1)
            def _():
                for g in narrow:
                    narrow_y(gbuf, 1, g).start()

        (make_normed if z == 0 else make_cotangent)()
        meet()
        for g, h in zip(wide, narrow):
            y_send[g].start()
            z_send[h].start()
        (narrow_n if z == 0 else narrow_g)()
        (make_cotangent if z == 0 else make_normed)()
        (narrow_g if z == 0 else narrow_n)()

        @pl.when(yb == 0)
        def _():
            for g in narrow:
                nbuf[g, 1] = jnp.zeros((tok, width), bf16)

        @pl.when(yb == 1)
        def _():
            for g in narrow:
                gbuf[g, 0] = jnp.zeros((tok, width), bf16)

        fetches[3].wait()

        @pl.loop(0, rows // CHUNK)
        def _(r):
            at = piece(r)
            for c in range(2):
                for h in range(2):
                    if z == 0:
                        col = c
                    elif h == 0:
                        col = 2 + c
                    else:
                        col = yb + 2 * c
                    start = col * tok
                    if not isinstance(start, int):
                        start = pl.multiple_of(start, tok)
                    block = mix_w[at, :, pl.ds(start, tok)].astype(f32)
                    keep = allowed(d * rows + r * CHUNK, col * tok, CHUNK, tok)
                    for g in range(h * hg, (h + 1) * hg):
                        w_send[g, at, c * tok : (c + 1) * tok] = jnp.where(
                            keep, block[:, g, :], 0.0
                        ).astype(bf16)

        for h in (z, 1 - z):
            go_mix[h].start()

            @pl.when(needs(h)(t_own))
            def _():
                w_at(h, d)[...] = w_send[h * hg : (h + 1) * hg]

        for i, g in enumerate(narrow):
            block = nt(gbuf[g, g_own[g]], nbuf[g, n_own[g]])
            kept = jnp.where(allowed(0, 0, tok, tok), block, 0.0).astype(bf16)
            for p in range(per_block):
                term_d[p, i] = kept[p * rows : (p + 1) * rows]
        terms_d.start()

        fetches[6].wait()
        own_bias = mix_bias[:, 0:tok]
        for b in range(1, QUAD):
            own_bias = jnp.where(k == b, mix_bias[:, b * tok : (b + 1) * tok], own_bias)
        for g in range(groups):
            bias_t[g] = jnp.transpose(jnp.broadcast_to(own_bias[g : g + 1], (128, tok)))
        acc_gain[...] = jnp.zeros_like(acc_gain)
        acc_shift[...] = jnp.zeros_like(acc_shift)
        sum_a[...] = jnp.zeros_like(sum_a)
        sum_b[...] = jnp.zeros_like(sum_b)
        grad_mix[...] = jnp.zeros_like(grad_mix)
        lines = hg * width // 128
        per_span = span // 128
        for g in range(groups):
            bias_sum = nt(jnp.ones((8, width), bf16), gbuf[g, g_own[g]])[0:1]
            for b in range(QUAD):
                shown = jnp.where(k == b, bias_sum, 0.0)
                for c in range(tok // 128):
                    at = 2 * lines + g * per_span + b * (tok // 128) + c
                    early_s[0, at : at + 1, :] = shown[:, c * 128 : (c + 1) * 128]

        def give_u(g, mixed):
            for c in range(width // 128):
                lanes = slice(c * 128, (c + 1) * 128)
                at = slice(g * width + c * 128, g * width + (c + 1) * 128)
                whole = (mixed[:, lanes] + bias_t[g]).astype(bf16).astype(f32)
                grad_u[:, at] = (upstream[:, at].astype(f32) * whole).astype(bf16)

        def give_back(g, total):
            back[g] = total.astype(bf16)

            @pl.loop(0, tok // CHUNK)
            def _(r):
                at = piece(r)
                grad_normed = back[g, at, :].astype(f32)
                one = unit[at, lanes_of(g)]
                prod = grad_normed * one
                acc_gain[:, lanes_of(g)] += prod[0:8] + prod[8:16]
                acc_shift[:, lanes_of(g)] += grad_normed[0:8] + grad_normed[8:16]
                scaled = grad_normed * gain[:, lanes_of(g)]
                prod = scaled * one
                a, b = scaled[:, 0:128], prod[:, 0:128]
                for c in range(1, width // 128):
                    a = a + scaled[:, c * 128 : (c + 1) * 128]
                    b = b + prod[:, c * 128 : (c + 1) * 128]
                sum_a[at, :] += a
                sum_b[at, :] += b

        def give_v():
            @pl.loop(0, tok // CHUNK)
            def _(r):
                at = piece(r)
                mean_a = jnp.sum(sum_a[at, :], axis=-1, keepdims=True) / half
                mean_b = jnp.sum(sum_b[at, :], axis=-1, keepdims=True) / half
                inv_std = inv[at, :][:, 0:1]
                for g in range(groups):
                    scaled = back[g, at, :].astype(f32) * gain[:, lanes_of(g)]
                    grad_v[at, lanes_of(g)] = (
                        inv_std * (scaled - mean_a - unit[at, lanes_of(g)] * mean_b)
                    ).astype(bf16)

        def own_cols(g, block):
            at = pl.ds(pl.multiple_of(block * tok, tok), tok)
            return w_block[:, g, :, at].reshape(2 * tok, tok)

        def own_rows(g, block):
            return w_block[pl.ds(block * per_block, per_block), g].reshape(tok, 2 * tok)

        def pair(buf, g):
            return buf[g].reshape(2 * tok, width)

        def keep_of(row, col):
            return allowed(row * tok, col * tok, tok, tok)

        def gather_sums(h, out):
            first = h * hg * width
            for ref, line in ((acc_gain, 0), (acc_shift, lines)):
                whole = jnp.sum(ref[:, first : first + hg * width], axis=0, keepdims=True)
                for i in range(lines):
                    out[0, line + i : line + i + 1, :] = whole[:, i * 128 : (i + 1) * 128]

        def send_early():
            gather_sums(1, early_s)
            early_go[0].start()
            early_a[d] = early_s[0]

        def spread_early():
            early_go[0].arrive()
            early_s[1] = total(lambda j: early_a.at[j], dp_count)
            early_go[1].start()
            early_c[me // 2] = early_s[1]

        def respread_early():
            early_go[1].arrive()
            early_s[2] = total(lambda j: early_c.at[j], spans * QUAD // 2)
            early_go[2].start()
            early_b[lax.rem(me, 2)] = early_s[2]

        def send_late():
            gather_sums(0, late_s)
            late_go[0].start()
            late_a[d] = late_s[0]

        def spread_late():
            late_go[0].arrive()
            late_s[1] = total(lambda j: late_a.at[j], dp_count)
            late_go[1].start()
            late_b[me] = late_s[1]

        def put_sums(h, whole):
            for i in range(lines):
                to = slice((h * lines + i) * 128, (h * lines + i + 1) * 128)
                grad_gain[:, to] = whole[i : i + 1]
                grad_shift[:, to] = whole[lines + i : lines + i + 1]

        def take_early():
            early_go[2].arrive()
            whole = total(lambda j: early_b.at[j], 2)
            put_sums(1, whole)
            for g in range(groups):
                for c in range(per_span):
                    at = 2 * lines + g * per_span + c
                    grad_bias[g : g + 1, c * 128 : (c + 1) * 128] = whole[at : at + 1]

        def take_late():
            late_go[1].arrive()
            put_sums(0, total(lambda j: late_b.at[j], spans * QUAD))

        go_mix[z].arrive()
        for i, g in enumerate(wide):
            y_take[g].wait_recv()
            if z == 0:
                both = nn(w_block[:, g].reshape(2 * tok, 2 * tok), pair(nbuf, g))
                stage_z[i] = both[tok:].astype(bf16)
                pz[i].start()
                give_u(g, both[:tok])
            else:
                both = tn(w_block[:, g].reshape(2 * tok, 2 * tok), pair(gbuf, g))
                stage_z[i] = both[:tok].astype(bf16)
                pz[i].start()
                give_back(g, both[tok:])
            z_take[g].wait_recv()
            if z == 0:
                stage_y[i] = tn(own_cols(g, 1 - yb), pair(gbuf, g)).astype(bf16)
            else:
                stage_y[i] = nn(own_rows(g, 1 - yb), pair(nbuf, g)).astype(bf16)
            if z == 0 or i < hg - 1:
                py[i].start()
            block = nt(pair(gbuf, g), pair(nbuf, g))
            for a in range(2):
                for b in range(2):
                    if z == 0:
                        keep = keep_of(yb + 2 * a, b)
                    else:
                        keep = keep_of(2 + a, yb + 2 * b)
                    at, of_s = slice(a * tok, (a + 1) * tok), slice(b * tok, (b + 1) * tok)
                    kept = jnp.where(keep, block[at, of_s], 0.0).astype(bf16)
                    for p in range(per_block):
                        term_w[a * per_block + p, i, :, of_s] = kept[p * rows : (p + 1) * rows]
            terms_w[i].start()
            if z == 0:
                own_part[i] = tn(own_cols(g, yb), pair(gbuf, g))
            else:
                own_part[i] = nn(own_rows(g, yb), pair(nbuf, g))

        go_mix[1 - z].arrive()
        terms_d.over_spans()
        for i, g in enumerate(narrow):
            terms_w[i].over_spans()

            @pl.when(yb == 1)
            def _():
                narrow_y(nbuf, 0, g).wait_recv()
                block = nt(gbuf[g, g_own[g]], nbuf[g, 0]).astype(bf16)
                for p in range(per_block):
                    term_l[p, i] = block[p * rows : (p + 1) * rows]

            @pl.when(yb == 0)
            def _():
                narrow_y(gbuf, 1, g).wait_recv()

            if i == hg - 1:
                terms_l.start()
            if z == 0:
                give_u(g, nn(own_rows(g, yb), pair(nbuf, g)))
            pz[i].wait_recv()
            if z == 0:
                give_back(g, recv_z[i].astype(f32) + tn(own_cols(g, yb), pair(gbuf, g)))
            else:
                give_back(g, tn(own_cols(g, yb), pair(gbuf, g)))
                give_u(g, recv_z[i].astype(f32) + nn(own_rows(g, yb), pair(nbuf, g)))

        send_early()
        if z == 1:
            send_late()
        for term in (terms_d, *terms_w):
            term.pass_round(along_y=z == 1)
        terms_l.over_spans()
        if z == 1:
            for term in (terms_d, *terms_w):
                term.relay_column()
            py[hg - 1].start()
        spread_early()
        if z == 1:
            spread_late()

        for i, g in enumerate(wide):
            if z == 1 and i == hg - 1:
                terms_l.pass_round()
                for term in (terms_d, *terms_w):
                    term.relay_row()
                respread_early()
                give_v()
            py[i].wait_recv()
            whole = own_part[i] + recv_y[i].astype(f32)
            if z == 0:
                give_back(g, whole)
            else:
                give_u(g, whole)
        if z == 0:
            send_late()
            for term in (*terms_w, terms_d):
                term.pass_along_y()
            terms_l.pass_round()
            respread_early()
            spread_late()
            terms_l.relay_column()
            give_v()
        else:
            terms_l.relay_column()

        def put(g, first, block):
            grad_mix[:, g, first * tok : first * tok + block.shape[1]] = block.astype(f32)

        for g in wide:
            y_send[g].wait_send()
        for g in narrow:
            z_send[g].wait_send()

            @pl.when(yb == 0)
            def _():
                narrow_y(nbuf, 0, g).wait_send()

            @pl.when(yb == 1)
            def _():
                narrow_y(gbuf, 1, g).wait_send()

        for i in range(hg):
            py[i].wait_send()
            pz[i].wait_send()
        for go in (*go_mix, late_go[0], early_go[0]):
            go.leave()

        terms_d.arrive()
        for t in range(QUAD):

            @pl.when(t_own == t)
            def _():
                for i in range(hg):
                    put(i if t >= 2 else hg + i, t, all_d[t, i])

        terms_d.leave()
        for i, term in enumerate(terms_w):
            term.arrive()
            put(i, 0, all_w[lax.rem(t_own, 2), i])

            @pl.when(t_own >= 2)
            def _():
                for b in range(2):
                    put(hg + i, b, all_w[2 + b, i][:, :tok])

            for t in range(2, QUAD):

                @pl.when(t_own == t)
                def _():
                    for b in range(t - 1):
                        put(hg + i, b + 2, all_w[2 + b, i][:, tok:])

            term.leave()
        terms_l.arrive()
        for t in range(1, QUAD, 2):

            @pl.when(t_own == t)
            def _():
                for i in range(hg):
                    put(i if t >= 2 else hg + i, t - 1, all_l[t, i])

        terms_l.leave()
        take_early()
        for go in early_go[1:]:
            go.leave()
        take_late()
        late_go[1].leave()

    for z in range(2):
        pl.when(zb == z)(functools.partial(run, z))


def finish(*refs):
    count = len(refs) // 2
    sems = refs[-1]
    copies = [
        pltpu.make_async_copy(src, dst, sems.at[i])
        for i, (src, dst) in enumerate(zip(refs[:count], refs[count : 2 * count]))
    ]
    for copy in copies:
        copy.start()
    for copy in copies:
        copy.wait()


def per_device(gated, values_in, upstream, gain, shift, mix_w, mix_bias):
    dp_count = lax.axis_size("dp")
    sp_count = lax.axis_size("sp")
    tok, half = gated.shape[1:]
    rows, groups, span = mix_w.shape
    width = half // groups
    assert span == QUAD * tok and groups % 2 == 0 and tok % rows == 0
    spans = sp_count // QUAD
    hg = groups // 2
    f32, bf16 = jnp.float32, jnp.bfloat16
    hbm = pl.BlockSpec(memory_space=pltpu.HBM)
    vmem = pl.BlockSpec(memory_space=pltpu.VMEM)
    dma = pltpu.SemaphoreType.DMA
    term, slim = (hg, rows, 2 * tok), (hg, rows, tok)
    late_rows = half // 128
    early_rows = late_rows + groups * span // 128
    assert half % 256 == 0 and tok % 128 == 0
    scratch = (
        [pltpu.VMEM((tok, half), bf16)] * 3
        + [
            pltpu.VMEM((rows, groups, span), bf16),
            pltpu.VMEM((1, half), f32),
            pltpu.VMEM((1, half), f32),
            pltpu.VMEM((groups, span), f32),
            pltpu.VMEM((tok, half), f32),
            pltpu.VMEM((tok, 128), f32),
            pltpu.VMEM((groups, 2, tok, width), bf16),
            pltpu.VMEM((groups, 2, tok, width), bf16),
            pltpu.VMEM((groups, rows, 2 * tok), bf16),
            pltpu.VMEM((2 * (tok // rows), groups, rows, 2 * tok), bf16),
        ]
        + [pltpu.VMEM((hg, tok, width), bf16)] * 4
        + [
            pltpu.VMEM((hg, tok, width), f32),
            pltpu.VMEM((groups, tok, width), bf16),
            pltpu.VMEM((tok, 128), f32),
            pltpu.VMEM((tok, 128), f32),
            pltpu.VMEM((8, half), f32),
            pltpu.VMEM((8, half), f32),
            pltpu.VMEM((2 * (tok // rows),) + term, bf16),
            pltpu.VMEM((tok // rows,) + slim, bf16),
            pltpu.VMEM((tok // rows,) + slim, bf16),
        ]
        + [pltpu.VMEM((hg, dp_count, rows, 2 * tok), bf16)]
        + [pltpu.VMEM((dp_count,) + shape, bf16) for shape in (slim, slim)]
        + [pltpu.VMEM(shape, bf16) for shape in (term, slim, slim)]
        + [pltpu.VMEM((spans,) + shape, bf16) for shape in (term, slim, slim)]
        + [pltpu.VMEM((QUAD,) + shape, bf16) for shape in (term, slim, slim)]
        + [
            pltpu.VMEM((2, late_rows, 128), f32),
            pltpu.VMEM((dp_count, late_rows, 128), f32),
            pltpu.VMEM((sp_count, late_rows, 128), f32),
            pltpu.VMEM((3, early_rows, 128), f32),
            pltpu.VMEM((dp_count, early_rows, 128), f32),
            pltpu.VMEM((2, early_rows, 128), f32),
            pltpu.VMEM((sp_count // 2, early_rows, 128), f32),
            pltpu.VMEM((groups, tok, 128), f32),
        ]
        + [dma((2, groups)), dma((4, hg)), dma((2, hg))]
        + [dma((4 + hg, dp_count - 1)), dma((2, dp_count - 1)), dma((2 + hg,)), dma((10,))]
        + [dma((2 + hg, spans - 1))] * 2
        + [dma((2 + hg, 4)), dma((2 + hg, 3))]
        + [dma((7,))]
    )
    shapes = (
        jax.ShapeDtypeStruct((tok, half), bf16),
        jax.ShapeDtypeStruct((tok, half), bf16),
        jax.ShapeDtypeStruct((rows, groups, span), f32),
        jax.ShapeDtypeStruct((1, half), f32),
        jax.ShapeDtypeStruct((1, half), f32),
        jax.ShapeDtypeStruct((groups, span), f32),
    )
    out = pl.pallas_call(
        functools.partial(kernel, (tok, width, groups, span, dp_count, spans)),
        out_shape=shapes,
        in_specs=[hbm] * 7,
        out_specs=[vmem] * 6,
        scratch_shapes=scratch,
        compiler_params=pltpu.CompilerParams(
            collective_id=0, has_side_effects=True, vmem_limit_bytes=36 * 1024 * 1024
        ),
    )(
        *(
            pltpu.with_memory_space_constraint(x, pltpu.HBM)
            for x in (
                gated[0],
                values_in[0],
                upstream[0],
                gain[None],
                shift[None],
                mix_w,
                mix_bias,
            )
        )
    )
    u, v, mix, gain_g, shift_g, bias = pl.pallas_call(
        finish,
        out_shape=shapes,
        in_specs=[vmem] * 6,
        out_specs=[hbm] * 6,
        scratch_shapes=[dma((6,))],
        compiler_params=pltpu.CompilerParams(vmem_limit_bytes=36 * 1024 * 1024),
    )(*out)
    return (u[None], v[None], mix, bias, gain_g[0], shift_g[0])


def solution(mesh):
    placed = (
        P("dp", "sp", None),
        P("dp", "sp", None),
        P("dp", "sp", None),
        P(),
        P(),
        P("dp", None, None),
        P(),
    )
    return jax.shard_map(
        per_device,
        mesh=mesh,
        in_specs=placed,
        out_specs=(P("dp", "sp", None), P("dp", "sp", None), P("dp", None, None), P(), P(), P()),
        check_vma=False,
    )
```

```python
import functools

import jax
import jax.numpy as jnp
from jax import lax
from jax.experimental import pallas as pl
from jax.experimental.pallas import tpu as pltpu
from jax.sharding import PartitionSpec as P

SEG = 64

EPS = 1e-05

CHUNK = 16

QUAD = 4


def nt(a, b):
    return lax.dot_general(a, b, (((1,), (1,)), ((), ())), preferred_element_type=jnp.float32)


def tn(a, b):
    return lax.dot_general(a, b, (((0,), (0,)), ((), ())), preferred_element_type=jnp.float32)


def nn(a, b):
    return jnp.dot(a, b, preferred_element_type=jnp.float32)


def kernel(
    dims,
    gated_in,
    values_in,
    upstream_in,
    gain_in,
    shift_in,
    mix_in,
    bias_in,
    grad_u,
    grad_v,
    grad_mix,
    grad_gain,
    grad_shift,
    grad_bias,
    gated,
    values,
    upstream,
    mix_w,
    gain,
    shift,
    mix_bias,
    unit,
    inv,
    nbuf,
    gbuf,
    w_send,
    w_block,
    stage_y,
    stage_z,
    recv_y,
    recv_z,
    own_part,
    back,
    sum_a,
    sum_b,
    acc_gain,
    acc_shift,
    term_w,
    term_d,
    term_l,
    red_w,
    red_d,
    red_l,
    dp_w,
    dp_d,
    dp_l,
    span_w,
    span_d,
    span_l,
    all_w,
    all_d,
    all_l,
    late_s,
    late_a,
    late_b,
    early_s,
    early_a,
    early_b,
    early_c,
    bias_t,
    raw_sems,
    part_sems,
    z_sems,
    dp_send,
    mix_recv,
    red_recv,
    vec_sems,
    sn_send,
    sn_recv,
    sq_send,
    sq_recv,
    in_sem,
):
    tok, width, groups, span, dp_count, spans = dims
    half = groups * width
    rows = span // dp_count
    per_block = tok // rows
    hg = groups // 2
    me = lax.axis_index("sp")
    my_span, k = me // QUAD, lax.rem(me, QUAD)
    zb, yb = k // 2, lax.rem(k, 2)
    d = lax.axis_index("dp")
    t_own = d // per_block
    f32, bf16 = jnp.float32, jnp.bfloat16

    def sq_id(j):
        return {"sp": my_span * QUAD + j}

    def dp_id(j):
        return {"dp": j}

    def sn_id(j):
        return {"sp": j * QUAD + k}

    def sp_id(j):
        return {"sp": j}

    y_id = sq_id(k + 1 - 2 * yb)
    z_id = sq_id(k + 2 - 4 * zb)

    def remote(src, dst, send, recv, where):
        return pltpu.make_async_remote_copy(
            src_ref=src,
            dst_ref=dst,
            send_sem=send,
            recv_sem=recv,
            device_id=where,
            device_id_type=pl.DeviceIdType.MESH,
        )

    class Exchange:
        def __init__(
            self, src, dst, own, count, where, send, recv, gives=None, takes=None, bulk=None
        ):
            self.src, self.dst, self.own, self.count = src, dst, own, count
            self.where, self.send, self.recv = where, send, recv
            self.gives, self.takes, self.bulk = gives, takes, bulk

        def copy(self, step, to):
            peer = lax.rem(self.own + step, self.count)
            landing = self.own if to else peer
            by = step if to else self.count - step
            return remote(
                self.src(peer) if to else self.dst(landing),
                self.dst(landing),
                self.send(step - 1),
                self.recv(by - 1),
                self.where(peer),
            )

        def each(self, cond, act):
            for step in range(1, self.count):
                if cond is None:
                    act(step)
                else:
                    pl.when(cond(lax.rem(self.own + step, self.count)))(lambda: act(step))

        def all_of_it(self):
            where = self.where(lax.rem(self.own + 1, self.count))
            return remote(self.bulk, self.bulk, self.send(0), self.recv(0), where)

        def start(self):
            self.each(self.gives, lambda step: self.copy(step, True).start())

        def arrive(self):
            if self.bulk is None:
                self.each(self.takes, lambda step: self.copy(step, False).wait_recv())
            elif self.takes is None:
                self.all_of_it().wait_recv()
            else:
                pl.when(self.takes(self.own))(lambda: self.all_of_it().wait_recv())

        def leave(self):
            if self.bulk is None or self.gives is not None:
                self.each(self.gives, lambda step: self.copy(step, True).wait_send())
            else:
                self.all_of_it().wait_send()

    def across(src, dst, send, recv, gives=None, takes=None, bulk=None):
        return Exchange(src, dst, d, dp_count, dp_id, send, recv, gives, takes, bulk)

    def spanning(src, dst, slot, gives=None, takes=None):
        return Exchange(
            src,
            dst,
            my_span,
            spans,
            sn_id,
            lambda step: sn_send.at[slot, step],
            lambda step: sn_recv.at[slot, step],
            gives,
            takes,
        )

    fetches = [
        pltpu.make_async_copy(src, dst, in_sem.at[i])
        for i, (src, dst) in enumerate(
            (
                (gated_in, gated),
                (upstream_in, upstream),
                (values_in, values),
                (mix_in, mix_w),
                (gain_in, gain),
                (shift_in, shift),
                (bias_in, mix_bias),
            )
        )
    ]
    for z, order in ((0, (4, 5, 2, 0, 1, 3, 6)), (1, (0, 1, 2, 4, 5, 3, 6))):

        @pl.when(zb == z)
        def _():
            for i in order:
                fetches[i].start()

    barrier = pltpu.get_barrier_semaphore()
    for own, count, where in ((me, spans * QUAD, sp_id), (d, dp_count, dp_id)):
        for step in range(1, count):
            pl.semaphore_signal(
                barrier,
                inc=1,
                device_id=where(lax.rem(own + step, count)),
                device_id_type=pl.DeviceIdType.MESH,
            )

    def piece(r):
        return pl.ds(pl.multiple_of(r * CHUNK, CHUNK), CHUNK)

    def lanes_of(g):
        return slice(g * width, (g + 1) * width)

    def allowed(first_t, first_s, n_t, n_s):
        t = first_t + lax.broadcasted_iota(jnp.int32, (n_t, n_s), 0)
        s = first_s + lax.broadcasted_iota(jnp.int32, (n_t, n_s), 1)
        return lax.div(t, SEG) >= lax.div(s, SEG)

    def run(z):
        first = range(hg)
        second = range(hg, groups)
        wide = first if z == 0 else second
        narrow = second if z == 0 else first
        n_own = {g: yb if (z == 0 or g in first) else 1 for g in range(groups)}
        g_own = {g: yb if (z == 1 or g in second) else 0 for g in range(groups)}

        def makes_w(t):
            return (lax.rem(t, 2) == yb) if z == 0 else (t >= 2)

        def slot_w(t):
            return lax.div(t, 2) if z == 0 else t - 2

        def makes_n(t):
            return t == k

        def of(j):
            return j // per_block

        def part(j):
            return lax.rem(j, per_block)

        x_buf = nbuf if z == 0 else gbuf
        o_buf = gbuf if z == 0 else nbuf
        raw_y = {}
        for g in wide:
            raw_y[g] = x_buf
        y_send = {
            g: remote(
                x_buf.at[g, yb], x_buf.at[g, yb], raw_sems.at[0, g], raw_sems.at[1, g], y_id
            )
            for g in wide
        }
        y_take = {
            g: remote(
                x_buf.at[g, 1 - yb],
                x_buf.at[g, 1 - yb],
                raw_sems.at[0, g],
                raw_sems.at[1, g],
                y_id,
            )
            for g in wide
        }

        def narrow_y(buf, slot, g):
            return remote(
                buf.at[g, slot], buf.at[g, slot], raw_sems.at[0, g], raw_sems.at[1, g], y_id
            )

        z_buf = nbuf if z == 0 else gbuf
        z_own = n_own if z == 0 else g_own
        z_slot = 0 if z == 0 else 1
        z_send = {
            g: remote(
                z_buf.at[g, z_own[g]],
                z_buf.at[g, z_slot],
                z_sems.at[0, i],
                z_sems.at[1, i],
                z_id,
            )
            for i, g in enumerate(narrow)
        }
        z_take = {
            g: remote(
                o_buf.at[g, 1 - z_slot],
                o_buf.at[g, 1 - z_slot],
                z_sems.at[0, i],
                z_sems.at[1, i],
                z_id,
            )
            for i, g in enumerate(wide)
        }
        py = [
            remote(stage_y.at[i], recv_y.at[i], part_sems.at[0, i], part_sems.at[1, i], y_id)
            for i in range(hg)
        ]
        pz = [
            remote(stage_z.at[i], recv_z.at[i], part_sems.at[2, i], part_sems.at[3, i], z_id)
            for i in range(hg)
        ]

        def needs(h):
            return makes_w if h == z else ((lambda t: t < 2) if z == 0 else (lambda t: t >= 2))

        def slot_of(h, t):
            return slot_w(t) if h == z else (t if z == 0 else t - 2)

        def w_at(h, j):
            return w_block.at[slot_of(h, of(j)) * per_block + part(j), h * hg : (h + 1) * hg]

        go_mix = [
            across(
                lambda j, h=h: w_send.at[h * hg : (h + 1) * hg],
                lambda j, h=h: w_at(h, j),
                lambda step, h=h: dp_send.at[h, step],
                lambda step, h=h: mix_recv.at[h, step],
                lambda j, h=h: needs(h)(t_own),
                lambda j, h=h: needs(h)(of(j)),
            )
            for h in range(2)
        ]
        def makes_l(t):
            return (t == k) & (yb == 1)

        def peer_w(j):
            return ((j < 2) & (lax.rem(t_own, 2) == j)) | ((j >= 2) & (t_own >= 2))

        def peer_d(j):
            return t_own == j

        def peer_l(j):
            return (t_own == j) & (lax.rem(j, 2) == 1)

        class Reduction:
            def __init__(self, makes, peer, source, refs, slot, passes):
                red, dp_sum, over, every, bulk = refs
                self.makes, self.refs, self.source = makes, refs, source
                self.to_dp = across(
                    source,
                    lambda j: red(j),
                    lambda step: dp_send.at[2 + slot, step],
                    lambda step: red_recv.at[slot],
                    lambda j: makes(of(j)),
                    lambda j: makes(t_own),
                    bulk,
                )
                self.to_span = spanning(
                    lambda j: dp_sum,
                    lambda j: over(j),
                    slot,
                    lambda j: makes(t_own),
                    lambda j: makes(t_own),
                )
                self.peer = peer
                row, column = k + 1 - 2 * yb, k + 2 - 4 * zb

                def copy(piece, at, where):
                    return remote(
                        every(piece),
                        every(piece),
                        sq_send.at[slot, at],
                        sq_recv.at[slot, at],
                        where,
                    )

                self.own_z = lambda: copy(k, 0, z_id)
                self.own_y = lambda: copy(k, 1, y_id)
                self.take_z = lambda: copy(column, 0, z_id)
                self.take_y = lambda: copy(row, 1, y_id)
                self.relays = {
                    "column": lambda: remote(
                        every(column),
                        every(column),
                        sq_send.at[slot, 2],
                        sq_recv.at[slot, 2],
                        y_id,
                    ),
                    "row": lambda: remote(
                        every(row), every(row), sq_send.at[slot, 3], sq_recv.at[slot, 2], z_id
                    ),
                }
                self.take_relay = lambda: copy(3 - k, 2, z_id)
                self.row, self.column, self.passes = row, column, passes

            def start(self):
                self.to_dp.start()

            def over_spans(self):
                red, dp_sum, over, every, _bulk = self.refs

                @pl.when(self.makes(t_own))
                def _():
                    red(d)[...] = self.source(d)[...]
                    self.to_dp.arrive()
                    dp_sum[...] = total(red, dp_count).astype(bf16)
                    self.to_span.start()
                    over(my_span)[...] = dp_sum[...]

            def pass_round(self, along_y=True):
                red, dp_sum, over, every, _bulk = self.refs

                @pl.when(self.makes(t_own))
                def _():
                    self.to_span.arrive()
                    every(k)[...] = total(over, spans).astype(bf16)
                    self.own_z().start()
                    if along_y:
                        self.own_y().start()

            def pass_along_y(self):
                pl.when(self.makes(t_own))(lambda: self.own_y().start())

            def relay_column(self):
                @pl.when(self.peer(self.column))
                def _():
                    self.take_z().wait_recv()
                    self.relays["column"]().start()

            def relay_row(self):
                @pl.when(self.peer(self.row))
                def _():
                    self.take_y().wait_recv()
                    self.relays["row"]().start()

            def arrive(self):
                if "column" not in self.passes:
                    pl.when(self.peer(self.column))(lambda: self.take_z().wait_recv())
                if "row" not in self.passes:
                    pl.when(self.peer(self.row))(lambda: self.take_y().wait_recv())
                pl.when(self.peer(3 - k))(lambda: self.take_relay().wait_recv())

            def leave(self):
                self.to_dp.leave()
                self.to_span.leave()

                @pl.when(self.makes(t_own))
                def _():
                    self.own_z().wait_send()
                    self.own_y().wait_send()

                for way in self.passes:
                    peer = self.column if way == "column" else self.row
                    pl.when(self.peer(peer))(lambda: self.relays[way]().wait_send())

        def total(at, count):
            out = at(0)[...].astype(f32)
            for i in range(1, count):
                out = out + at(i)[...].astype(f32)
            return out

        terms_w = [
            Reduction(
                makes_w,
                peer_w,
                lambda j, i=i: term_w.at[slot_w(of(j)) * per_block + part(j), i],
                (
                    lambda j, i=i: red_w.at[i, j],
                    dp_w.at[i],
                    lambda j, i=i: span_w.at[j, i],
                    lambda j, i=i: all_w.at[j, i],
                    red_w.at[i, : dp_count - 1],
                ),
                i,
                ("column", "row") if z == 1 else (),
            )
            for i in range(hg)
        ]
        terms_d = Reduction(
            makes_n,
            peer_d,
            lambda j: term_d.at[part(j)],
            (
                lambda j: red_d.at[j],
                dp_d,
                lambda j: span_d.at[j],
                lambda j: all_d.at[j],
                red_d.at[: dp_count - 1],
            ),
            hg,
            ("column", "row") if z == 1 else (),
        )
        terms_l = Reduction(
            makes_l,
            peer_l,
            lambda j: term_l.at[part(j)],
            (
                lambda j: red_l.at[j],
                dp_l,
                lambda j: span_l.at[j],
                lambda j: all_l.at[j],
                red_l.at[: dp_count - 1],
            ),
            hg + 1,
            ("column",),
        )

        def vec(at):
            return lambda step: vec_sems.at[at]

        late_go = (
            across(
                lambda j: late_s.at[0],
                lambda j: late_a.at[j],
                lambda step: in_sem.at[0],
                vec(0),
                bulk=late_a.at[: dp_count - 1],
            ),
            Exchange(
                lambda j: late_s.at[1],
                lambda j: late_b.at[j],
                me,
                spans * QUAD,
                sp_id,
                lambda step: in_sem.at[1],
                vec(1),
                bulk=late_b.at[: spans * QUAD - 1],
            ),
        )
        early_go = (
            across(
                lambda j: early_s.at[0],
                lambda j: early_a.at[j],
                lambda step: in_sem.at[2],
                vec(2),
                bulk=early_a.at[: dp_count - 1],
            ),
            Exchange(
                lambda j: early_s.at[1],
                lambda j: early_c.at[j],
                me // 2,
                spans * QUAD // 2,
                lambda j: {"sp": 2 * j + lax.rem(me, 2)},
                lambda step: in_sem.at[3],
                vec(3),
                bulk=early_c.at[: spans * QUAD // 2 - 1],
            ),
            Exchange(
                lambda j: early_s.at[2],
                lambda j: early_b.at[j],
                lax.rem(me, 2),
                2,
                lambda j: {"sp": me - lax.rem(me, 2) + j},
                lambda step: in_sem.at[4],
                vec(4),
            ),
        )

        def make_normed():
            for fetch in (fetches[4], fetches[5], fetches[2]):
                fetch.wait()

            @pl.loop(0, tok // CHUNK, unroll=8)
            def _(r):
                at = piece(r)
                raw = values[at, :].astype(f32)
                centred = raw - jnp.mean(raw, axis=-1, keepdims=True)
                inv_std = lax.rsqrt(jnp.mean(centred * centred, axis=-1, keepdims=True) + EPS)
                one = centred * inv_std
                unit[at, :] = one
                inv[at, :] = jnp.broadcast_to(inv_std, (CHUNK, 128))
                normed = (one * gain[...] + shift[...]).astype(bf16)
                for g in range(groups):
                    nbuf[g, n_own[g], at, :] = normed[:, lanes_of(g)]

        def make_cotangent():
            fetches[0].wait()
            fetches[1].wait()

            @pl.loop(0, tok // CHUNK)
            def _(r):
                at = piece(r)
                prod = (upstream[at, :].astype(f32) * gated[at, :].astype(f32)).astype(bf16)
                for g in range(groups):
                    gbuf[g, g_own[g], at, :] = prod[:, lanes_of(g)]

        def meet():
            pl.semaphore_wait(barrier, spans * QUAD + dp_count - 2)

        def narrow_n():
            @pl.when(yb == 0)
            def _():
                for g in narrow:
                    narrow_y(nbuf, 0, g).start()

        def narrow_g():
            @pl.when(yb == 1)
            def _():
                for g in narrow:
                    narrow_y(gbuf, 1, g).start()

        (make_normed if z == 0 else make_cotangent)()
        meet()
        for g, h in zip(wide, narrow):
            y_send[g].start()
            z_send[h].start()
        (narrow_n if z == 0 else narrow_g)()
        (make_cotangent if z == 0 else make_normed)()
        (narrow_g if z == 0 else narrow_n)()

        @pl.when(yb == 0)
        def _():
            for g in narrow:
                nbuf[g, 1] = jnp.zeros((tok, width), bf16)

        @pl.when(yb == 1)
        def _():
            for g in narrow:
                gbuf[g, 0] = jnp.zeros((tok, width), bf16)

        fetches[3].wait()

        @pl.loop(0, rows // CHUNK)
        def _(r):
            at = piece(r)
            for c in range(2):
                for h in range(2):
                    if z == 0:
                        col = c
                    elif h == 0:
                        col = 2 + c
                    else:
                        col = yb + 2 * c
                    start = col * tok
                    if not isinstance(start, int):
                        start = pl.multiple_of(start, tok)
                    block = mix_w[at, :, pl.ds(start, tok)].astype(f32)
                    keep = allowed(d * rows + r * CHUNK, col * tok, CHUNK, tok)
                    for g in range(h * hg, (h + 1) * hg):
                        w_send[g, at, c * tok : (c + 1) * tok] = jnp.where(
                            keep, block[:, g, :], 0.0
                        ).astype(bf16)

        for h in (z, 1 - z):
            go_mix[h].start()

            @pl.when(needs(h)(t_own))
            def _():
                w_at(h, d)[...] = w_send[h * hg : (h + 1) * hg]

        for i, g in enumerate(narrow):
            block = nt(gbuf[g, g_own[g]], nbuf[g, n_own[g]])
            kept = jnp.where(allowed(0, 0, tok, tok), block, 0.0).astype(bf16)
            for p in range(per_block):
                term_d[p, i] = kept[p * rows : (p + 1) * rows]
        terms_d.start()

        fetches[6].wait()
        own_bias = mix_bias[:, 0:tok]
        for b in range(1, QUAD):
            own_bias = jnp.where(k == b, mix_bias[:, b * tok : (b + 1) * tok], own_bias)
        for g in range(groups):
            bias_t[g] = jnp.transpose(jnp.broadcast_to(own_bias[g : g + 1], (128, tok)))
        acc_gain[...] = jnp.zeros_like(acc_gain)
        acc_shift[...] = jnp.zeros_like(acc_shift)
        sum_a[...] = jnp.zeros_like(sum_a)
        sum_b[...] = jnp.zeros_like(sum_b)
        grad_mix[...] = jnp.zeros_like(grad_mix)
        lines = hg * width // 128
        per_span = span // 128
        for g in range(groups):
            bias_sum = nt(jnp.ones((8, width), bf16), gbuf[g, g_own[g]])[0:1]
            for b in range(QUAD):
                shown = jnp.where(k == b, bias_sum, 0.0)
                for c in range(tok // 128):
                    at = 2 * lines + g * per_span + b * (tok // 128) + c
                    early_s[0, at : at + 1, :] = shown[:, c * 128 : (c + 1) * 128]

        def give_u(g, mixed):
            for c in range(width // 128):
                lanes = slice(c * 128, (c + 1) * 128)
                at = slice(g * width + c * 128, g * width + (c + 1) * 128)
                whole = (mixed[:, lanes] + bias_t[g]).astype(bf16).astype(f32)
                grad_u[:, at] = (upstream[:, at].astype(f32) * whole).astype(bf16)

        def give_back(g, total):
            back[g] = total.astype(bf16)

            @pl.loop(0, tok // CHUNK)
            def _(r):
                at = piece(r)
                grad_normed = back[g, at, :].astype(f32)
                one = unit[at, lanes_of(g)]
                prod = grad_normed * one
                acc_gain[:, lanes_of(g)] += prod[0:8] + prod[8:16]
                acc_shift[:, lanes_of(g)] += grad_normed[0:8] + grad_normed[8:16]
                scaled = grad_normed * gain[:, lanes_of(g)]
                prod = scaled * one
                a, b = scaled[:, 0:128], prod[:, 0:128]
                for c in range(1, width // 128):
                    a = a + scaled[:, c * 128 : (c + 1) * 128]
                    b = b + prod[:, c * 128 : (c + 1) * 128]
                sum_a[at, :] += a
                sum_b[at, :] += b

        def give_v():
            @pl.loop(0, tok // CHUNK)
            def _(r):
                at = piece(r)
                mean_a = jnp.sum(sum_a[at, :], axis=-1, keepdims=True) / half
                mean_b = jnp.sum(sum_b[at, :], axis=-1, keepdims=True) / half
                inv_std = inv[at, :][:, 0:1]
                for g in range(groups):
                    scaled = back[g, at, :].astype(f32) * gain[:, lanes_of(g)]
                    grad_v[at, lanes_of(g)] = (
                        inv_std * (scaled - mean_a - unit[at, lanes_of(g)] * mean_b)
                    ).astype(bf16)

        def own_cols(g, block):
            at = pl.ds(pl.multiple_of(block * tok, tok), tok)
            return w_block[:, g, :, at].reshape(2 * tok, tok)

        def own_rows(g, block):
            return w_block[pl.ds(block * per_block, per_block), g].reshape(tok, 2 * tok)

        def pair(buf, g):
            return buf[g].reshape(2 * tok, width)

        def keep_of(row, col):
            return allowed(row * tok, col * tok, tok, tok)

        def gather_sums(h, out):
            first = h * hg * width
            for ref, line in ((acc_gain, 0), (acc_shift, lines)):
                whole = jnp.sum(ref[:, first : first + hg * width], axis=0, keepdims=True)
                for i in range(lines):
                    out[0, line + i : line + i + 1, :] = whole[:, i * 128 : (i + 1) * 128]

        def send_early():
            gather_sums(1, early_s)
            early_go[0].start()
            early_a[d] = early_s[0]

        def spread_early():
            early_go[0].arrive()
            early_s[1] = total(lambda j: early_a.at[j], dp_count)
            early_go[1].start()
            early_c[me // 2] = early_s[1]

        def respread_early():
            early_go[1].arrive()
            early_s[2] = total(lambda j: early_c.at[j], spans * QUAD // 2)
            early_go[2].start()
            early_b[lax.rem(me, 2)] = early_s[2]

        def send_late():
            gather_sums(0, late_s)
            late_go[0].start()
            late_a[d] = late_s[0]

        def spread_late():
            late_go[0].arrive()
            late_s[1] = total(lambda j: late_a.at[j], dp_count)
            late_go[1].start()
            late_b[me] = late_s[1]

        def put_sums(h, whole):
            for i in range(lines):
                to = slice((h * lines + i) * 128, (h * lines + i + 1) * 128)
                grad_gain[:, to] = whole[i : i + 1]
                grad_shift[:, to] = whole[lines + i : lines + i + 1]

        def take_early():
            early_go[2].arrive()
            whole = total(lambda j: early_b.at[j], 2)
            put_sums(1, whole)
            for g in range(groups):
                for c in range(per_span):
                    at = 2 * lines + g * per_span + c
                    grad_bias[g : g + 1, c * 128 : (c + 1) * 128] = whole[at : at + 1]

        def take_late():
            late_go[1].arrive()
            put_sums(0, total(lambda j: late_b.at[j], spans * QUAD))

        go_mix[z].arrive()
        for i, g in enumerate(wide):
            y_take[g].wait_recv()
            if z == 0:
                both = nn(w_block[:, g].reshape(2 * tok, 2 * tok), pair(nbuf, g))
                stage_z[i] = both[tok:].astype(bf16)
                pz[i].start()
                give_u(g, both[:tok])
            else:
                both = tn(w_block[:, g].reshape(2 * tok, 2 * tok), pair(gbuf, g))
                stage_z[i] = both[:tok].astype(bf16)
                pz[i].start()
                give_back(g, both[tok:])
            z_take[g].wait_recv()
            if z == 0:
                stage_y[i] = tn(own_cols(g, 1 - yb), pair(gbuf, g)).astype(bf16)
            else:
                stage_y[i] = nn(own_rows(g, 1 - yb), pair(nbuf, g)).astype(bf16)
            if z == 0 or i < hg - 1:
                py[i].start()
            block = nt(pair(gbuf, g), pair(nbuf, g))
            for a in range(2):
                for b in range(2):
                    if z == 0:
                        keep = keep_of(yb + 2 * a, b)
                    else:
                        keep = keep_of(2 + a, yb + 2 * b)
                    at, of_s = slice(a * tok, (a + 1) * tok), slice(b * tok, (b + 1) * tok)
                    kept = jnp.where(keep, block[at, of_s], 0.0).astype(bf16)
                    for p in range(per_block):
                        term_w[a * per_block + p, i, :, of_s] = kept[p * rows : (p + 1) * rows]
            terms_w[i].start()
            if z == 0:
                own_part[i] = tn(own_cols(g, yb), pair(gbuf, g))
            else:
                own_part[i] = nn(own_rows(g, yb), pair(nbuf, g))

        go_mix[1 - z].arrive()
        terms_d.over_spans()
        for i, g in enumerate(narrow):
            terms_w[i].over_spans()

            @pl.when(yb == 1)
            def _():
                narrow_y(nbuf, 0, g).wait_recv()
                block = nt(gbuf[g, g_own[g]], nbuf[g, 0]).astype(bf16)
                for p in range(per_block):
                    term_l[p, i] = block[p * rows : (p + 1) * rows]

            @pl.when(yb == 0)
            def _():
                narrow_y(gbuf, 1, g).wait_recv()

            if i == hg - 1:
                terms_l.start()
            if z == 0:
                give_u(g, nn(own_rows(g, yb), pair(nbuf, g)))
            pz[i].wait_recv()
            if z == 0:
                give_back(g, recv_z[i].astype(f32) + tn(own_cols(g, yb), pair(gbuf, g)))
            else:
                give_back(g, tn(own_cols(g, yb), pair(gbuf, g)))
                give_u(g, recv_z[i].astype(f32) + nn(own_rows(g, yb), pair(nbuf, g)))

        send_early()
        if z == 1:
            send_late()
        for term in (terms_d, *terms_w):
            term.pass_round(along_y=z == 1)
        terms_l.over_spans()
        if z == 1:
            for term in (terms_d, *terms_w):
                term.relay_column()
            py[hg - 1].start()
        spread_early()
        if z == 1:
            spread_late()

        for i, g in enumerate(wide):
            if z == 1 and i == hg - 1:
                terms_l.pass_round()
                for term in (terms_d, *terms_w):
                    term.relay_row()
                respread_early()
                give_v()
            py[i].wait_recv()
            whole = own_part[i] + recv_y[i].astype(f32)
            if z == 0:
                give_back(g, whole)
            else:
                give_u(g, whole)
        if z == 0:
            send_late()
            for term in (*terms_w, terms_d):
                term.pass_along_y()
            terms_l.pass_round()
            respread_early()
            spread_late()
            terms_l.relay_column()
            give_v()
        else:
            terms_l.relay_column()

        def put(g, first, block):
            grad_mix[:, g, first * tok : first * tok + block.shape[1]] = block.astype(f32)

        for g in wide:
            y_send[g].wait_send()
        for g in narrow:
            z_send[g].wait_send()

            @pl.when(yb == 0)
            def _():
                narrow_y(nbuf, 0, g).wait_send()

            @pl.when(yb == 1)
            def _():
                narrow_y(gbuf, 1, g).wait_send()

        for i in range(hg):
            py[i].wait_send()
            pz[i].wait_send()
        for go in (*go_mix, late_go[0], early_go[0]):
            go.leave()

        terms_d.arrive()
        for t in range(QUAD):

            @pl.when(t_own == t)
            def _():
                for i in range(hg):
                    put(i if t >= 2 else hg + i, t, all_d[t, i])

        for i, term in enumerate(terms_w):
            term.arrive()
            put(i, 0, all_w[lax.rem(t_own, 2), i])

            @pl.when(t_own >= 2)
            def _():
                for b in range(2):
                    put(hg + i, b, all_w[2 + b, i][:, :tok])

            for t in range(2, QUAD):

                @pl.when(t_own == t)
                def _():
                    for b in range(t - 1):
                        put(hg + i, b + 2, all_w[2 + b, i][:, tok:])

        terms_l.arrive()
        for t in range(1, QUAD, 2):

            @pl.when(t_own == t)
            def _():
                for i in range(hg):
                    put(i if t >= 2 else hg + i, t - 1, all_l[t, i])

        take_early()
        for go in early_go[1:]:
            go.leave()
        take_late()
        late_go[1].leave()
        for term in (terms_d, *terms_w, terms_l):
            term.leave()

    for z in range(2):
        pl.when(zb == z)(functools.partial(run, z))


def finish(*refs):
    count = len(refs) // 2
    sems = refs[-1]
    copies = [
        pltpu.make_async_copy(src, dst, sems.at[i])
        for i, (src, dst) in enumerate(zip(refs[:count], refs[count : 2 * count]))
    ]
    for copy in copies:
        copy.start()
    for copy in copies:
        copy.wait()


def per_device(gated, values_in, upstream, gain, shift, mix_w, mix_bias):
    dp_count = lax.axis_size("dp")
    sp_count = lax.axis_size("sp")
    tok, half = gated.shape[1:]
    rows, groups, span = mix_w.shape
    width = half // groups
    assert span == QUAD * tok and groups % 2 == 0 and tok % rows == 0
    spans = sp_count // QUAD
    hg = groups // 2
    f32, bf16 = jnp.float32, jnp.bfloat16
    hbm = pl.BlockSpec(memory_space=pltpu.HBM)
    vmem = pl.BlockSpec(memory_space=pltpu.VMEM)
    dma = pltpu.SemaphoreType.DMA
    term, slim = (hg, rows, 2 * tok), (hg, rows, tok)
    late_rows = half // 128
    early_rows = late_rows + groups * span // 128
    assert half % 256 == 0 and tok % 128 == 0
    scratch = (
        [pltpu.VMEM((tok, half), bf16)] * 3
        + [
            pltpu.VMEM((rows, groups, span), bf16),
            pltpu.VMEM((1, half), f32),
            pltpu.VMEM((1, half), f32),
            pltpu.VMEM((groups, span), f32),
            pltpu.VMEM((tok, half), f32),
            pltpu.VMEM((tok, 128), f32),
            pltpu.VMEM((groups, 2, tok, width), bf16),
            pltpu.VMEM((groups, 2, tok, width), bf16),
            pltpu.VMEM((groups, rows, 2 * tok), bf16),
            pltpu.VMEM((2 * (tok // rows), groups, rows, 2 * tok), bf16),
        ]
        + [pltpu.VMEM((hg, tok, width), bf16)] * 4
        + [
            pltpu.VMEM((hg, tok, width), f32),
            pltpu.VMEM((groups, tok, width), bf16),
            pltpu.VMEM((tok, 128), f32),
            pltpu.VMEM((tok, 128), f32),
            pltpu.VMEM((8, half), f32),
            pltpu.VMEM((8, half), f32),
            pltpu.VMEM((2 * (tok // rows),) + term, bf16),
            pltpu.VMEM((tok // rows,) + slim, bf16),
            pltpu.VMEM((tok // rows,) + slim, bf16),
        ]
        + [pltpu.VMEM((hg, dp_count, rows, 2 * tok), bf16)]
        + [pltpu.VMEM((dp_count,) + shape, bf16) for shape in (slim, slim)]
        + [pltpu.VMEM(shape, bf16) for shape in (term, slim, slim)]
        + [pltpu.VMEM((spans,) + shape, bf16) for shape in (term, slim, slim)]
        + [pltpu.VMEM((QUAD,) + shape, bf16) for shape in (term, slim, slim)]
        + [
            pltpu.VMEM((2, late_rows, 128), f32),
            pltpu.VMEM((dp_count, late_rows, 128), f32),
            pltpu.VMEM((sp_count, late_rows, 128), f32),
            pltpu.VMEM((3, early_rows, 128), f32),
            pltpu.VMEM((dp_count, early_rows, 128), f32),
            pltpu.VMEM((2, early_rows, 128), f32),
            pltpu.VMEM((sp_count // 2, early_rows, 128), f32),
            pltpu.VMEM((groups, tok, 128), f32),
        ]
        + [dma((2, groups)), dma((4, hg)), dma((2, hg))]
        + [dma((4 + hg, dp_count - 1)), dma((2, dp_count - 1)), dma((2 + hg,)), dma((5,))]
        + [dma((2 + hg, spans - 1))] * 2
        + [dma((2 + hg, 4)), dma((2 + hg, 3))]
        + [dma((7,))]
    )
    shapes = (
        jax.ShapeDtypeStruct((tok, half), bf16),
        jax.ShapeDtypeStruct((tok, half), bf16),
        jax.ShapeDtypeStruct((rows, groups, span), f32),
        jax.ShapeDtypeStruct((1, half), f32),
        jax.ShapeDtypeStruct((1, half), f32),
        jax.ShapeDtypeStruct((groups, span), f32),
    )
    out = pl.pallas_call(
        functools.partial(kernel, (tok, width, groups, span, dp_count, spans)),
        out_shape=shapes,
        in_specs=[hbm] * 7,
        out_specs=[vmem] * 6,
        scratch_shapes=scratch,
        compiler_params=pltpu.CompilerParams(
            collective_id=0, has_side_effects=True, vmem_limit_bytes=36 * 1024 * 1024
        ),
    )(
        *(
            pltpu.with_memory_space_constraint(x, pltpu.HBM)
            for x in (
                gated[0],
                values_in[0],
                upstream[0],
                gain[None],
                shift[None],
                mix_w,
                mix_bias,
            )
        )
    )
    u, v, mix, gain_g, shift_g, bias = pl.pallas_call(
        finish,
        out_shape=shapes,
        in_specs=[vmem] * 6,
        out_specs=[hbm] * 6,
        scratch_shapes=[dma((6,))],
        compiler_params=pltpu.CompilerParams(vmem_limit_bytes=36 * 1024 * 1024),
    )(*out)
    return (u[None], v[None], mix, bias, gain_g[0], shift_g[0])


def solution(mesh):
    placed = (
        P("dp", "sp", None),
        P("dp", "sp", None),
        P("dp", "sp", None),
        P(),
        P(),
        P("dp", None, None),
        P(),
    )
    return jax.shard_map(
        per_device,
        mesh=mesh,
        in_specs=placed,
        out_specs=(P("dp", "sp", None), P("dp", "sp", None), P("dp", None, None), P(), P(), P()),
        check_vma=False,
    )
```
